32 devices in a mesh: grp: 2 (over x), row: 4 (over z), col: 4 (over y, core).
Axes of the slice: x: 2, y: 2, z: 4, core: 2. Of those that a mesh axis runs over, the one named last changes fastest.
Arguments:
- gate_in: bfloat16 [8, 512, 1024], P(('grp', 'row'), 'col'), parts along dimension 0, may hold values from -6 to 6
- mult_in: bfloat16 [8, 512, 1024], P(('grp', 'row'), 'col'), parts along dimension 0, may hold values from -6 to 6
- value_in: bfloat16 [8, 512, 1024], P(('grp', 'row'), 'col'), parts along dimension 0, may hold values from -6 to 6
- taps_gate: float32 [3, 1024], replicated, may hold values from -3.5 to 3.5
- taps_mult: float32 [3, 1024], replicated, may hold values from -3.5 to 3.5
- taps_value: float32 [3, 1024], replicated, may hold values from -3.5 to 3.5
- filter_first: float32 [33, 128], replicated, may hold values from -3 to 3
- filter_second: float32 [128, 128], replicated, may hold values from -1 to 1
- filter_ahead: float32 [128, 1024], replicated, may hold values from -0.5 to 0.5
- filter_behind: float32 [128, 1024], replicated, may hold values from -0.5 to 0.5
- filter_decay: float32 [1024], replicated, may hold values from 0.05 to 17.033333
- skip_gain: float32 [1024], replicated, may hold values from -5 to 5
- out_weight: bfloat16 [1024, 2048], replicated, may hold values from -0.1875 to 0.1875
Outputs:
- mixed: bfloat16 [8, 512, 2048], P(('grp', 'row'), 'col'), parts along dimension 0
The draws below stay inside these ranges and needn't reach their ends.
There are 2 independent parts, one for each index of `grp`. The reference program is written for one: setup_inputs(seed, part) draws one part's arguments, and reference() takes and returns one part's arrays. A program takes and returns all parts, laid end to end along the dimension named above; an argument that names none is the same for every part. Nothing has to cross between parts.
All inputs are finite; a program needn't handle non-finite values.
Results may differ from the reference program's by a relative error of at most 0.0049.
Values may be sent and summed in bfloat16 or wider, within the bound.
A program may use at most 64 MiB of HBM per device.

```python
import math
import jax
import jax.numpy as jnp
from jax import lax

D = 2048
H = 1024
FH = 128
FEAT = 33
TAPS = 3
SEQ = 512
SEQS = 4


def draw_filter_decay(key, part):
    slow_key, fast_key, pick_key = jax.random.split(jax.random.fold_in(key, 7), 3)
    slow_rates = jnp.exp(jax.random.uniform(slow_key, (H,), jnp.float32, math.log(0.05), math.log(2.0)))
    fast_rates = (SEQ - 1) / jnp.exp(jax.random.uniform(fast_key, (H,), jnp.float32, math.log(30.0), math.log(100.0)))
    fast_share = 0.5
    chosen = jax.random.uniform(pick_key, (H,), jnp.float32) < fast_share
    return jnp.where(chosen, fast_rates, slow_rates)


def block_levels(key, shape, shards, low, high):
    level = 1.0
    for axis_at, parts in shards:
        heights = jax.random.uniform(jax.random.fold_in(jax.random.fold_in(key, 6), axis_at), (parts,), jnp.float32, low / len(shards), high / len(shards))
        level = level * jnp.repeat(jnp.exp(heights), shape[axis_at] // parts).reshape((-1,) + (1,) * (len(shape) - 1 - axis_at))
    return level


def gaussian(rng, extent, deviation, reach, cuts=(), kind=jnp.bfloat16):
    loudness = block_levels(rng, extent, cuts, -0.22, 0.18) if cuts else 1.0
    values = jax.random.normal(rng, extent, jnp.float32) * deviation * loudness
    return jnp.minimum(jnp.maximum(values, -reach), reach).astype(kind)


def setup_inputs(seed: int = 0, part: int = 0) -> dict:
    keys = jax.random.split(jax.random.key(seed), 14)
    own_keys = jax.random.split(jax.random.fold_in(keys[13], part), 14)
    return {
        "gate_in": gaussian(own_keys[0], (SEQS, SEQ, H), 1.0, 6.0, ((0, 4), (1, 4))),
        "mult_in": gaussian(own_keys[1], (SEQS, SEQ, H), 1.0, 6.0, ((0, 4), (1, 4))),
        "value_in": gaussian(own_keys[2], (SEQS, SEQ, H), 1.0, 6.0, ((0, 4), (1, 4))),
        "taps_gate": gaussian(keys[3], (TAPS, H), TAPS ** -0.5, 3.5, (), jnp.float32),
        "taps_mult": gaussian(keys[4], (TAPS, H), TAPS ** -0.5, 3.5, (), jnp.float32),
        "taps_value": gaussian(keys[5], (TAPS, H), TAPS ** -0.5, 3.5, (), jnp.float32),
        "filter_first": jnp.clip(jax.random.uniform(keys[6], (FEAT, FH), jnp.float32, -3.0, 3.0), -3.0, 3.0),
        "filter_second": jnp.clip(jax.random.uniform(keys[7], (FH, FH), jnp.float32, -1.0, 1.0), -1.0, 1.0),
        "filter_ahead": gaussian(keys[8], (FH, H), FH ** -0.5, 0.5, (), jnp.float32),
        "filter_behind": gaussian(keys[9], (FH, H), FH ** -0.5, 0.5, (), jnp.float32),
        "filter_decay": draw_filter_decay(jax.random.fold_in(keys[13], 71), part),
        "skip_gain": gaussian(keys[11], (H,), 1.0, 5.0, (), jnp.float32),
        "out_weight": gaussian(keys[12], (H, D), H ** -0.5, 0.1875),
    }


highest = lax.Precision.HIGHEST

def filter_hidden(mirror, seq_len, filter_first, filter_second):
    tau_values = mirror.astype(jnp.float32) / (seq_len - 1)
    omega_pos = 2.0 * math.pi / seq_len * mirror.astype(jnp.float32)
    band_count = (filter_first.shape[0] - 1) // 2
    band_values = jnp.linspace(0.0001, band_count - 1, band_count, dtype=jnp.float32)
    angles = omega_pos[:, None] * band_values[None, :]
    features = jnp.concatenate([tau_values[:, None], jnp.cos(angles), -jnp.sin(angles)], axis=1)
    hidden = jnp.sin(jnp.dot(features, filter_first, precision=highest))
    hidden = jnp.sin(jnp.dot(hidden, filter_second, precision=highest))
    return (hidden, tau_values)

def side_values(hidden, tau_values, side_weight, decay_rates):
    values = jnp.einsum('pf,fh->hp', hidden, side_weight, precision=highest)
    return values * jnp.exp(-decay_rates[:, None] * tau_values[None, :])

def short_conv(source, tap_weights):
    seq_len = source.shape[0]
    padded = jnp.pad(source.astype(jnp.float32), ((1, 1), (0, 0)))
    summed = jnp.zeros(source.shape, jnp.float32)
    for offset in range(tap_weights.shape[0]):
        summed = summed + tap_weights[offset] * padded[offset:offset + seq_len]
    return summed

def reference(gate_in, mult_in, value_in, taps_gate, taps_mult, taps_value, filter_first, filter_second, filter_ahead, filter_behind, filter_decay, skip_gain, out_weight):
    seq_len = gate_in.shape[1]
    span_len = 2 * seq_len
    mirror = jnp.arange(seq_len, dtype=jnp.int32)
    hidden, tau_values = filter_hidden(mirror, seq_len, filter_first, filter_second)
    ahead_vals = side_values(hidden, tau_values, filter_ahead, filter_decay)
    behind_vals = side_values(hidden, tau_values, filter_behind, filter_decay)
    kernel = jnp.concatenate([ahead_vals, jnp.zeros((ahead_vals.shape[0], 1), jnp.float32), jnp.flip(behind_vals[:, 1:], axis=1)], axis=1)
    kernel = kernel * lax.rsqrt(lax.optimization_barrier(jnp.sum(kernel * kernel, axis=1, keepdims=True)) + 1e-06)
    kernel_freq = jnp.fft.rfft(kernel, n=span_len, axis=1)

    def one_sequence(inputs):
        gate_rows, mult_rows, value_rows = inputs
        gate_part = short_conv(gate_rows, taps_gate)
        product = short_conv(value_rows, taps_value) * short_conv(mult_rows, taps_mult)
        spectrum = jnp.fft.rfft(product.T, n=span_len, axis=1)
        convolved = jnp.fft.irfft(spectrum * kernel_freq, n=span_len, axis=1)[:, :seq_len].T
        mixed_rows = ((convolved + skip_gain * product) * gate_part).astype(jnp.bfloat16)
        return jnp.dot(mixed_rows, out_weight, preferred_element_type=jnp.float32).astype(jnp.bfloat16)
    return lax.map(one_sequence, (gate_in, mult_in, value_in))
```

```python
import functools
import math

import jax
import jax.numpy as jnp
import numpy as np
from jax import lax
from jax.experimental import pallas as pl
from jax.experimental.pallas import tpu as pltpu
from jax.sharding import PartitionSpec as P

highest = lax.Precision.HIGHEST


def padded_2(shard, sides, width):
    for axis, dim in sides:
        size, length = (lax.axis_size(axis), shard.shape[dim])
        up = [(i, (i + 1) % size) for i in range(size - 1)]
        down = [(j, i) for i, j in up]
        last = lax.slice_in_dim(shard, length - width, length, axis=dim)
        leading = lax.slice_in_dim(shard, 0, width, axis=dim)
        before = lax.ppermute(last, axis, up)
        after = lax.ppermute(leading, axis, down)
        shard = jnp.concatenate([before, shard, after], axis=dim)
    return shard


def filter_hidden(mirror, seq_len, filter_first, filter_second):
    tau_values = mirror.astype(jnp.float32) / (seq_len - 1)
    omega_pos = 2.0 * math.pi / seq_len * mirror.astype(jnp.float32)
    band_count = (filter_first.shape[0] - 1) // 2
    band_values = jnp.linspace(0.0001, band_count - 1, band_count, dtype=jnp.float32)
    angles = omega_pos[:, None] * band_values[None, :]
    features = jnp.concatenate([tau_values[:, None], jnp.cos(angles), -jnp.sin(angles)], axis=1)
    hidden = jnp.sin(jnp.dot(features, filter_first, precision=highest))
    hidden = jnp.sin(jnp.dot(hidden, filter_second, precision=highest))
    return (hidden, tau_values)


def side_values(hidden, tau_values, side_weight, decay_rates):
    values = jnp.einsum("pf,fh->hp", hidden, side_weight, precision=highest)
    return values * jnp.exp(-decay_rates[:, None] * tau_values[None, :])


def angle_table(row_count, column_count, period):
    products = (
        lax.iota(jnp.int32, row_count)[:, None]
        * lax.iota(jnp.int32, column_count)[None, :]
        % period
    )
    angle = products.astype(jnp.float32) * (2.0 * math.pi / period)
    return (jnp.cos(angle), jnp.sin(angle))


def swap_halves(stacked, width):
    return jnp.concatenate([stacked[..., width:], stacked[..., :width]], axis=-1)


def forward(values, first_table, twist_even, twist_odd, second_block):
    channels, _, width = values.shape
    first = jnp.einsum("sfa,cab->cfsb", first_table, values, precision=highest)
    first = first.reshape(channels, first_table.shape[1], 2 * width)
    turned = first * twist_even + swap_halves(first, width) * twist_odd
    return jnp.einsum("cfk,kl->cfl", turned, second_block, precision=highest)


def inverse(spectrum, last_table, twist_even, twist_odd, second_block, span_len):
    channels, freq_rows, double_width = spectrum.shape
    width = double_width // 2
    back = jnp.einsum("cfk,kl->cfl", spectrum, second_block, precision=highest)
    turned = back * twist_even + swap_halves(back, width) * twist_odd
    turned = turned.reshape(channels, freq_rows, 2, width)
    result = jnp.einsum("asf,cfsb->cab", last_table, turned, precision=highest)
    return result / span_len


def spread_body(
    gate_in,
    mult_in,
    value_in,
    taps_gate,
    taps_mult,
    taps_value,
    filter_first,
    filter_second,
    filter_ahead,
    filter_behind,
    filter_decay,
    skip_gain,
    out_weight,
):
    col_count = lax.axis_size("col")
    col_index = lax.axis_index("col")
    tok_rows = gate_in.shape[1]
    seq_len = tok_rows * col_count
    span_len = 2 * seq_len
    group_size = filter_ahead.shape[1] // col_count
    stacked = jnp.stack([gate_in[0], mult_in[0], value_in[0]])
    padded = padded_2(stacked, (("col", 1),), 1).astype(jnp.float32)
    all_taps = jnp.stack([taps_gate, taps_mult, taps_value])
    shorted = jnp.zeros(stacked.shape, jnp.float32)
    for offset in range(all_taps.shape[1]):
        shorted = shorted + all_taps[:, offset][:, None, :] * padded[:, offset : offset + tok_rows]
    gate_part = shorted[0]
    product = shorted[2] * shorted[1]
    spread = lax.all_to_all(product.T, "col", split_axis=0, concat_axis=1, tiled=True)
    first_channel = col_index * group_size
    own_rates = lax.dynamic_slice_in_dim(filter_decay, first_channel, group_size)
    mirror = lax.iota(jnp.int32, seq_len)
    hidden, tau_values = filter_hidden(mirror, seq_len, filter_first, filter_second)
    ahead_vals = side_values(
        hidden,
        tau_values,
        lax.dynamic_slice_in_dim(filter_ahead, first_channel, group_size, 1),
        own_rates,
    )
    behind_vals = side_values(
        hidden,
        tau_values,
        lax.dynamic_slice_in_dim(filter_behind, first_channel, group_size, 1),
        own_rates,
    )
    kernel = jnp.concatenate(
        [ahead_vals, jnp.zeros((group_size, 1), jnp.float32), jnp.flip(behind_vals[:, 1:], axis=1)],
        axis=1,
    )
    kernel = kernel * lax.rsqrt(jnp.sum(kernel * kernel, axis=1, keepdims=True) + 1e-06)
    factor = 128
    half_rows = factor // 2
    width_second = span_len // factor
    first_cos, first_sin = angle_table(factor, factor, factor)
    twist_cos, twist_sin = angle_table(factor, width_second, span_len)
    second_cos, second_sin = angle_table(width_second, width_second, width_second)
    first_table = jnp.stack([first_cos, -first_sin])
    last_table = jnp.stack([first_cos[:half_rows], -first_sin[:half_rows]], axis=1)
    twist_even = jnp.concatenate([twist_cos, twist_cos], axis=1)
    twist_ahead = jnp.concatenate([twist_sin, -twist_sin], axis=1)
    twist_back = jnp.concatenate([-twist_sin, twist_sin], axis=1)
    block_ahead = jnp.concatenate(
        [
            jnp.concatenate([second_cos, -second_sin], axis=1),
            jnp.concatenate([second_sin, second_cos], axis=1),
        ],
        axis=0,
    )
    block_back = jnp.concatenate(
        [
            jnp.concatenate([second_cos, second_sin], axis=1),
            jnp.concatenate([-second_sin, second_cos], axis=1),
        ],
        axis=0,
    )
    kernel_spec = forward(
        kernel.reshape(group_size, factor, width_second),
        first_table,
        twist_even,
        twist_ahead,
        block_ahead,
    )
    data_spec = forward(
        spread.reshape(group_size, half_rows, width_second),
        first_table[:, :, :half_rows],
        twist_even,
        twist_ahead,
        block_ahead,
    )
    data_re = data_spec[..., :width_second]
    data_im = data_spec[..., width_second:]
    kernel_re = kernel_spec[..., :width_second]
    kernel_im = kernel_spec[..., width_second:]
    joined = jnp.concatenate(
        [data_re * kernel_re - data_im * kernel_im, data_re * kernel_im + data_im * kernel_re],
        axis=-1,
    )
    convolved = inverse(joined, last_table, twist_even, twist_back, block_back, span_len).reshape(
        group_size, seq_len
    )
    returned = lax.all_to_all(convolved, "col", split_axis=1, concat_axis=0, tiled=True)
    mixed_rows = ((returned.T + skip_gain * product) * gate_part).astype(jnp.bfloat16)
    return jnp.dot(mixed_rows, out_weight, preferred_element_type=jnp.float32).astype(jnp.bfloat16)[
        None
    ]


f32, bf16 = (jnp.float32, jnp.bfloat16)
EDGE = 16
PARTS = 2
LANES = 128
FEATS = 64


def halves(table):
    high = table.astype(bf16)
    return [high, (table - high.astype(np.float64)).astype(bf16)]


def wave_tables(seq_len):
    odd = 2 * np.arange(seq_len, dtype=np.int64) + 1
    low = odd[: seq_len // 2]
    angle = (low[:, None] * odd[None, :] % (8 * seq_len)) * (math.pi / (4 * seq_len))
    table = np.concatenate([np.cos(angle), np.sin(angle)], axis=0)
    half = low * (math.pi / (4 * seq_len))
    turn = np.stack([np.cos(half), np.sin(half)]).astype(np.float32)
    turn = np.repeat(turn[:, :, None], LANES, axis=2)
    return (np.stack(halves(table)), np.stack(halves(table.T)), turn)


def feature_table(seq_len, feature_count):
    position = np.arange(seq_len, dtype=np.float64)
    bands = (feature_count - 1) // 2
    values = np.linspace(0.0001, bands - 1, bands)
    angles = (2.0 * math.pi / seq_len * position)[:, None] * values[None, :]
    tau = position / (seq_len - 1)
    table = np.concatenate([tau[:, None], np.cos(angles), -np.sin(angles)], axis=1)
    return np.concatenate(halves(np.pad(table, ((0, 0), (0, FEATS - feature_count)))), axis=1)


def sine(x):
    turns = jnp.floor(x * (1.0 / math.pi) + 0.5)
    r = x - turns * 3.140625
    r = r - turns * 9.67502593994140625e-4
    r = r - turns * 1.509957990978376432e-7
    sign = 1.0 - 2.0 * (turns - 2.0 * jnp.floor(turns * 0.5))
    s = r * r
    poly = 1.0 / 362880.0 - s * (1.0 / 39916800.0)
    poly = -1.0 / 5040.0 + s * poly
    poly = 1.0 / 120.0 + s * poly
    poly = -1.0 / 6.0 + s * poly
    return sign * (r + r * s * poly)


def split(value):
    high = value.astype(bf16)
    return (high, (value - high.astype(f32)).astype(bf16))


def mul(a, b):
    return jnp.dot(a, b, preferred_element_type=f32)


def joined(value, axis):
    return jnp.concatenate(split(value), axis=axis)


def twice(weight):
    both = joined(weight, 1)
    return jnp.concatenate([both, both], axis=0)


def neighbours(rows, before, after):
    count = rows.shape[0]
    index = lax.broadcasted_iota(jnp.int32, rows.shape, 0)
    up = jnp.where(index == 0, before, pltpu.roll(rows, 1, 0))
    down = jnp.where(index == count - 1, after, pltpu.roll(rows, count - 1, 0))
    return (up, down)


def short_form(rows, taps, before, after):
    up, down = neighbours(rows, before, after)
    return taps[0:1] * up + taps[1:2] * rows + taps[2:3] * down


def conv_kernel(
    n,
    gate_hbm,
    mult_hbm,
    value_hbm,
    taps_gate_hbm,
    taps_mult_hbm,
    taps_value_hbm,
    first_hbm,
    second_hbm,
    ahead_hbm,
    behind_hbm,
    decay_hbm,
    skip_hbm,
    weight_hbm,
    table_hbm,
    table_t_hbm,
    turn_hbm,
    feature_hbm,
    out_ref,
    gate,
    mult,
    value,
    taps_gate,
    taps_mult,
    taps_value,
    second_ref,
    decay_ref,
    skip_ref,
    first,
    ahead_w,
    behind_w,
    weight,
    table,
    table_t,
    turn,
    feature,
    sent,
    came,
    whole,
    back_sent,
    back_came,
    halo_sent,
    halo_came,
    kernel_re,
    kernel_im,
    spec,
    gate_part,
    direct,
    total,
    load_sems,
    lead_sems,
    send_sems,
    recv_sems,
    back_send,
    back_recv,
    halo_send,
    halo_recv,
):
    me = lax.axis_index("col")
    rows, channels = gate.shape
    group = channels // n
    seq_len = rows * n
    half = seq_len // 2
    near = me + 1 - 2 * lax.rem(me, 2)
    peers = []
    for j in range(1, n // 2):
        peers += [lax.rem(me + 2 * j, n), lax.rem(near + 2 * j, n)]
    peers.append(near)
    order = peers + [me]

    barrier = pltpu.get_barrier_semaphore()
    for peer in peers:
        pl.semaphore_signal(
            barrier, inc=1, device_id={"col": peer}, device_id_type=pl.DeviceIdType.MESH
        )

    def columns(owner):
        return pl.ds(pl.multiple_of(owner * group, group), group)

    def load(src, dst, sem):
        copy = pltpu.make_async_copy(src, dst, sem)
        copy.start()
        return copy

    tap_loads = [
        load(taps_value_hbm, taps_value, load_sems.at[0]),
        load(taps_mult_hbm, taps_mult, load_sems.at[1]),
    ]
    lead = []
    for i, owner in enumerate(order):
        cols = columns(owner)
        lead.append(
            [
                load(value_hbm.at[0, :, cols], value.at[:, cols], lead_sems.at[0, i]),
                load(mult_hbm.at[0, :, cols], mult.at[:, cols], lead_sems.at[1, i]),
            ]
        )
    loads = {}
    for i, (name, s, d) in enumerate(
        [
            ("feature", feature_hbm, feature),
            ("first", first_hbm, first.at[pl.ds(0, first_hbm.shape[0])]),
            ("second", second_hbm, second_ref),
            ("decay", decay_hbm, decay_ref),
            ("ahead", ahead_hbm.at[:, columns(me)], ahead_w),
            ("behind", behind_hbm.at[:, columns(me)], behind_w),
            ("gate", gate_hbm.at[0], gate),
        ]
    ):
        loads[name] = load(s, d, load_sems.at[2 + i])

    part = group // PARTS

    def piece(owner, h):
        return pl.ds(pl.multiple_of(owner * group + h * part, part), part)

    def pack(owner, h):
        cols = piece(owner, h)
        v = value[:, cols].astype(f32)
        m = mult[:, cols].astype(f32)
        zero = jnp.zeros((1, part), f32)
        vs = short_form(v, taps_value[:, cols], zero, zero)
        ms = short_form(m, taps_mult[:, cols], zero, zero)
        sent[h, owner, pl.ds(0, rows), :] = (vs * ms).astype(bf16)
        edges = jnp.concatenate(
            [v[0:2], v[rows - 2 : rows], m[0:2], m[rows - 2 : rows], jnp.zeros((8, part), f32)], axis=0
        )
        sent[h, owner, pl.ds(rows, EDGE), :] = edges.astype(bf16)

    def remote(src, dst, ssem, rsem, peer):
        return pltpu.make_async_remote_copy(
            src_ref=src,
            dst_ref=dst,
            send_sem=ssem,
            recv_sem=rsem,
            device_id={"col": peer},
            device_id_type=pl.DeviceIdType.MESH,
        )

    copies = []
    for copy in tap_loads:
        copy.wait()
    for h in range(PARTS):
        for i, peer in enumerate(peers):
            if h == 0:
                for copy in lead[i]:
                    copy.wait()
            pack(peer, h)
            if i + h == 0:
                pl.semaphore_wait(barrier, n - 1)
            copy = remote(
                sent.at[h, peer], came.at[h, me], send_sems.at[h, peer], recv_sems.at[h, me], peer
            )
            copy.start()
            copies.append(copy)
    for i, (name, s, d) in enumerate(
        [
            ("table", table_hbm, table),
            ("turn", turn_hbm, turn),
            ("table_t", table_t_hbm, table_t),
            ("taps_gate", taps_gate_hbm, taps_gate),
            ("skip", skip_hbm, skip_ref),
            ("weight", weight_hbm, weight),
        ]
    ):
        loads[name] = load(s, d, load_sems.at[9 + i])
    for copy in lead[n - 1]:
        copy.wait()
    loads["gate"].wait()
    right, left = (lax.rem(me + 1, n), lax.rem(me + n - 1, n))
    slabs = channels // LANES
    for side, (row, target) in enumerate([(rows - 1, right), (0, left)]):
        base = rows - EDGE if row else 0
        at = row - base
        parts = []
        for r in (gate, mult, value):
            line = r[base : base + EDGE, :].astype(f32)[at : at + 1]
            parts.append(
                jnp.concatenate([line[:, b * LANES : (b + 1) * LANES] for b in range(slabs)], axis=0)
            )
        halo_sent[side] = jnp.concatenate(parts, axis=1).astype(bf16)
        copy = remote(
            halo_sent.at[side], halo_came.at[side], halo_send.at[side], halo_recv.at[side], target
        )
        copy.start()
        copies.append(copy)
    for h in range(PARTS):
        pack(me, h)

    def signs(shape):
        return (1 - 2 * (lax.broadcasted_iota(jnp.int32, shape, 0) % 2)).astype(f32)

    for name in ("feature", "first", "second"):
        loads[name].wait()
    used = first_hbm.shape[0]
    at = lax.broadcasted_iota(jnp.int32, first.shape, 0)
    wide = mul(feature[...], twice(jnp.where(at < used, first[...], 0.0)))
    hidden = sine(wide[:, :LANES] + wide[:, LANES:])
    wide = mul(joined(hidden, 1), twice(second_ref[...]))
    hidden = sine(wide[:, :LANES] + wide[:, LANES:])
    row_at = lax.broadcasted_iota(jnp.int32, hidden.shape, 0)
    later = jnp.where(row_at == seq_len - 1, 0.0, pltpu.roll(hidden, seq_len - 1, 0))
    for name in ("decay", "ahead", "behind"):
        loads[name].wait()
    rates = decay_ref[:, columns(me)] * (-1.0 / (seq_len - 1))
    index = lax.broadcasted_iota(jnp.int32, (seq_len, group), 0)
    fade = jnp.exp(rates * index.astype(f32))

    def side(values, w):
        high, low = split(w)
        return mul(values, jnp.concatenate([high, high], axis=0)) + mul(
            values, jnp.concatenate([low, low], axis=0)
        )

    ahead = side(joined(hidden, 1), ahead_w[...])
    behind = side(joined(later, 1), behind_w[...] * jnp.exp(rates))
    sums = (ahead + behind) * fade
    gaps = (ahead - behind) * fade
    power = jnp.sum(sums * sums + gaps * gaps, axis=0, keepdims=True) * 0.5
    scale = lax.rsqrt(power + 1e-06) * (2.0 / (2 * seq_len))
    flip = signs((seq_len, part)).astype(bf16)
    for name in ("table", "turn"):
        loads[name].wait()
    cos_half = turn[0][:, 0:1]
    sin_half = turn[1][:, 0:1]
    for h in range(PARTS):
        cols = slice(h * part, (h + 1) * part)
        sh, sl = split(sums[:, cols])
        gh, gl = split(gaps[:, cols])

        def turned(rows_at, a, b):
            high = jnp.concatenate([a[0], b[0] * flip], axis=1)
            low = jnp.concatenate([a[1], b[1] * flip], axis=1)
            t0 = table[0, rows_at : rows_at + half, :]
            t1 = table[1, rows_at : rows_at + half, :]
            return mul(t0, high) + mul(t1, high) + mul(t0, low)

        top = turned(0, (sh, sl), (gh, gl))
        bottom = turned(half, (gh, gl), (sh, sl))
        kernel_re[h] = cos_half * top + sin_half * bottom
        kernel_im[h] = sin_half * top - cos_half * bottom

    def near_product(h):
        whole[h, pl.ds(pl.multiple_of(me * rows, rows), rows), :part] = sent[h, me, pl.ds(0, rows), :]
        came[h, me, pl.ds(rows, EDGE), :] = sent[h, me, pl.ds(rows, EDGE), :]
        for peer in reversed(peers):
            remote(
                sent.at[h, peer], came.at[h, peer], send_sems.at[h, peer], recv_sems.at[h, peer], peer
            ).wait_recv()
            whole[h, pl.ds(pl.multiple_of(peer * rows, rows), rows), :part] = came[
                h, peer, pl.ds(0, rows), :
            ]
        edges = [came[h, s, pl.ds(rows, EDGE), :].astype(f32) for s in range(n)]
        own_taps = [t[:, piece(me, h)] for t in (taps_value, taps_mult)]
        tile_at = lax.broadcasted_iota(jnp.int32, (EDGE, part), 0)
        for s in range(n):
            top = bottom = 1.0
            for k, taps in enumerate(own_taps):
                e = edges[s][4 * k : 4 * k + 4]
                first_row = taps[1:2] * e[0:1] + taps[2:3] * e[1:2]
                last_row = taps[0:1] * e[2:3] + taps[1:2] * e[3:4]
                if s > 0:
                    first_row += taps[0:1] * edges[s - 1][4 * k + 3 : 4 * k + 4]
                if s < n - 1:
                    last_row += taps[2:3] * edges[s + 1][4 * k : 4 * k + 1]
                top, bottom = (top * first_row, bottom * last_row)
            for base, at, row in ((s * rows, 0, top), ((s + 1) * rows - EDGE, EDGE - 1, bottom)):
                old = whole[h, base : base + EDGE, :part].astype(f32)
                whole[h, base : base + EDGE, :part] = jnp.where(tile_at == at, row, old).astype(bf16)

    alternate = signs((rows, part))

    def invert(owner, h):
        take = pl.ds(pl.multiple_of(owner * rows, rows), rows)
        both = mul(table_t[0, take, :], spec[h])
        back = both[:, :part] + alternate * both[:, part:]
        return back * scale[:, h * part : (h + 1) * part]

    loads["table_t"].wait()
    for h in range(PARTS):
        near_product(h)
        whole[h, :, part:] = whole[h, :, :part] * flip
        freq = mul(table[0], whole[h])
        top, bottom = (freq[:half], freq[half:])
        kr, ki = (kernel_re[h], kernel_im[h])
        spec[h, :half] = (top * kr + bottom * ki).astype(bf16)
        spec[h, half:] = (bottom * kr - top * ki).astype(bf16)
        for peer in peers:
            back_sent[h, peer] = invert(peer, h).astype(bf16)
            copy = remote(
                back_sent.at[h, peer],
                back_came.at[h, me],
                back_send.at[h, peer],
                back_recv.at[h, me],
                peer,
            )
            copy.start()
            copies.append(copy)
    own_back = jnp.concatenate([invert(me, h) for h in range(PARTS)], axis=1)

    for side, target in enumerate((left, right)):
        remote(
            halo_sent.at[side], halo_came.at[side], halo_send.at[side], halo_recv.at[side], target
        ).wait_recv()
    for name in ("taps_gate", "skip"):
        loads[name].wait()
    has_left = (me > 0).astype(f32)
    has_right = (me < n - 1).astype(f32)
    befores = halo_came[0].astype(f32) * has_left
    afters = halo_came[1].astype(f32) * has_right

    def line(halo, i, s):
        lanes = slice(i * LANES, (i + 1) * LANES)
        blocks = range(s * group // LANES, (s + 1) * group // LANES)
        return jnp.concatenate([halo[b : b + 1, lanes] for b in blocks], axis=1)

    for s in range(n):
        cols = slice(s * group, (s + 1) * group)
        parts = []
        for i, (r, taps) in enumerate(((gate, taps_gate), (mult, taps_mult), (value, taps_value))):
            parts.append(
                short_form(r[:, cols].astype(f32), taps[:, cols], line(befores, i, s), line(afters, i, s))
            )
        gate_part[s] = parts[0]
        direct[s] = skip_ref[:, cols] * (parts[1] * parts[2])
    loads["weight"].wait()

    def project(owner, convolved):
        gated = ((convolved + direct[owner]) * gate_part[owner]).astype(bf16)
        return mul(gated, weight[columns(owner), :])

    total[...] = project(me, own_back)
    for i, peer in enumerate(reversed(peers)):
        for h in range(PARTS):
            remote(
                back_sent.at[h, peer],
                back_came.at[h, peer],
                back_send.at[h, peer],
                back_recv.at[h, peer],
                peer,
            ).wait_recv()
        arrived = [back_came[h, peer].astype(f32) for h in range(PARTS)]
        term = project(peer, jnp.concatenate(arrived, axis=1))
        if i < n - 2:
            total[...] += term
        else:
            out_ref[0] = (total[...] + term).astype(bf16)
    for copy in copies:
        copy.wait_send()


def fused_body(n, *args):
    gate_in, mult_in, value_in, tg, tm, tv, first, second, ahead, behind, decay, skip, weight = args
    _, rows, channels = gate_in.shape
    seq_len, group = (rows * n, channels // n)
    width = weight.shape[1]
    part = group // PARTS
    slabs = channels // LANES
    table, table_t, turn = wave_tables(seq_len)
    features = feature_table(seq_len, first.shape[0])
    vmem = pl.BlockSpec(memory_space=pltpu.VMEM)
    main = pl.BlockSpec(memory_space=pltpu.HBM)
    hidden_count = second.shape[0]
    dma = pltpu.SemaphoreType.DMA
    return pl.pallas_call(
        functools.partial(conv_kernel, n),
        out_shape=pltpu.VMEM((1, rows, width), bf16),
        in_specs=[main] * 17,
        out_specs=vmem,
        scratch_shapes=[
            pltpu.VMEM((rows, channels), bf16),
            pltpu.VMEM((rows, channels), bf16),
            pltpu.VMEM((rows, channels), bf16),
            pltpu.VMEM(tg.shape, f32),
            pltpu.VMEM(tm.shape, f32),
            pltpu.VMEM(tv.shape, f32),
            pltpu.VMEM(second.shape, f32),
            pltpu.VMEM((1, channels), f32),
            pltpu.VMEM((1, channels), f32),
            pltpu.VMEM((FEATS, hidden_count), f32),
            pltpu.VMEM((hidden_count, group), f32),
            pltpu.VMEM((hidden_count, group), f32),
            pltpu.VMEM(weight.shape, bf16),
            pltpu.VMEM(table.shape, bf16),
            pltpu.VMEM(table_t.shape, bf16),
            pltpu.VMEM(turn.shape, f32),
            pltpu.VMEM(features.shape, bf16),
            pltpu.VMEM((PARTS, n, rows + EDGE, part), bf16),
            pltpu.VMEM((PARTS, n, rows + EDGE, part), bf16),
            pltpu.VMEM((PARTS, seq_len, 2 * part), bf16),
            pltpu.VMEM((PARTS, n, rows, part), bf16),
            pltpu.VMEM((PARTS, n, rows, part), bf16),
            pltpu.VMEM((2, slabs, 3 * LANES), bf16),
            pltpu.VMEM((2, slabs, 3 * LANES), bf16),
            pltpu.VMEM((PARTS, seq_len // 2, 2 * part), f32),
            pltpu.VMEM((PARTS, seq_len // 2, 2 * part), f32),
            pltpu.VMEM((PARTS, seq_len, 2 * part), bf16),
            pltpu.VMEM((n, rows, group), f32),
            pltpu.VMEM((n, rows, group), f32),
            pltpu.VMEM((rows, width), f32),
            dma((15,)),
            dma((2, n)),
            dma((PARTS, n)),
            dma((PARTS, n)),
            dma((PARTS, n)),
            dma((PARTS, n)),
            dma((2,)),
            dma((2,)),
        ],
        compiler_params=pltpu.CompilerParams(
            collective_id=0, has_side_effects=True, vmem_limit_bytes=61 * 1024 * 1024
        ),
    )(
        gate_in, mult_in, value_in, tg, tm, tv, first, second, ahead, behind,
        decay.reshape(1, channels), skip.reshape(1, channels), weight,
        jnp.asarray(table), jnp.asarray(table_t), jnp.asarray(turn), jnp.asarray(features),
    )


def body_for(n, *args):
    _, rows, channels = args[0].shape
    small = rows * n <= 1024 and rows % 128 == 0 and channels % (128 * PARTS * n) == 0
    network = args[6].shape[0] <= FEATS and args[6].shape[1] == 128
    if n >= 2 and n % 2 == 0 and small and network and args[3].shape[0] == 3:
        return fused_body(n, *args)
    return spread_body(*args)


def solution(mesh):
    in_specs = (
        P(("grp", "row"), "col", None),
        P(("grp", "row"), "col", None),
        P(("grp", "row"), "col", None),
        P(),
        P(),
        P(),
        P(),
        P(),
        P(),
        P(),
        P(),
        P(),
        P(),
    )
    out_specs = P(("grp", "row"), "col", None)

    body = functools.partial(body_for, mesh.shape["col"])
    return jax.shard_map(body, mesh=mesh, in_specs=in_specs, out_specs=out_specs, check_vma=False)
```

```python
import functools
import math

import jax
import jax.numpy as jnp
import numpy as np
from jax import lax
from jax.experimental import pallas as pl
from jax.experimental.pallas import tpu as pltpu
from jax.sharding import PartitionSpec as P

highest = lax.Precision.HIGHEST


def padded_2(shard, sides, width):
    for axis, dim in sides:
        size, length = (lax.axis_size(axis), shard.shape[dim])
        up = [(i, (i + 1) % size) for i in range(size - 1)]
        down = [(j, i) for i, j in up]
        last = lax.slice_in_dim(shard, length - width, length, axis=dim)
        leading = lax.slice_in_dim(shard, 0, width, axis=dim)
        before = lax.ppermute(last, axis, up)
        after = lax.ppermute(leading, axis, down)
        shard = jnp.concatenate([before, shard, after], axis=dim)
    return shard


def filter_hidden(mirror, seq_len, filter_first, filter_second):
    tau_values = mirror.astype(jnp.float32) / (seq_len - 1)
    omega_pos = 2.0 * math.pi / seq_len * mirror.astype(jnp.float32)
    band_count = (filter_first.shape[0] - 1) // 2
    band_values = jnp.linspace(0.0001, band_count - 1, band_count, dtype=jnp.float32)
    angles = omega_pos[:, None] * band_values[None, :]
    features = jnp.concatenate([tau_values[:, None], jnp.cos(angles), -jnp.sin(angles)], axis=1)
    hidden = jnp.sin(jnp.dot(features, filter_first, precision=highest))
    hidden = jnp.sin(jnp.dot(hidden, filter_second, precision=highest))
    return (hidden, tau_values)


def side_values(hidden, tau_values, side_weight, decay_rates):
    values = jnp.einsum("pf,fh->hp", hidden, side_weight, precision=highest)
    return values * jnp.exp(-decay_rates[:, None] * tau_values[None, :])


def angle_table(row_count, column_count, period):
    products = (
        lax.iota(jnp.int32, row_count)[:, None]
        * lax.iota(jnp.int32, column_count)[None, :]
        % period
    )
    angle = products.astype(jnp.float32) * (2.0 * math.pi / period)
    return (jnp.cos(angle), jnp.sin(angle))


def swap_halves(stacked, width):
    return jnp.concatenate([stacked[..., width:], stacked[..., :width]], axis=-1)


def forward(values, first_table, twist_even, twist_odd, second_block):
    channels, _, width = values.shape
    first = jnp.einsum("sfa,cab->cfsb", first_table, values, precision=highest)
    first = first.reshape(channels, first_table.shape[1], 2 * width)
    turned = first * twist_even + swap_halves(first, width) * twist_odd
    return jnp.einsum("cfk,kl->cfl", turned, second_block, precision=highest)


def inverse(spectrum, last_table, twist_even, twist_odd, second_block, span_len):
    channels, freq_rows, double_width = spectrum.shape
    width = double_width // 2
    back = jnp.einsum("cfk,kl->cfl", spectrum, second_block, precision=highest)
    turned = back * twist_even + swap_halves(back, width) * twist_odd
    turned = turned.reshape(channels, freq_rows, 2, width)
    result = jnp.einsum("asf,cfsb->cab", last_table, turned, precision=highest)
    return result / span_len


def spread_body(
    gate_in,
    mult_in,
    value_in,
    taps_gate,
    taps_mult,
    taps_value,
    filter_first,
    filter_second,
    filter_ahead,
    filter_behind,
    filter_decay,
    skip_gain,
    out_weight,
):
    col_count = lax.axis_size("col")
    col_index = lax.axis_index("col")
    tok_rows = gate_in.shape[1]
    seq_len = tok_rows * col_count
    span_len = 2 * seq_len
    group_size = filter_ahead.shape[1] // col_count
    stacked = jnp.stack([gate_in[0], mult_in[0], value_in[0]])
    padded = padded_2(stacked, (("col", 1),), 1).astype(jnp.float32)
    all_taps = jnp.stack([taps_gate, taps_mult, taps_value])
    shorted = jnp.zeros(stacked.shape, jnp.float32)
    for offset in range(all_taps.shape[1]):
        shorted = shorted + all_taps[:, offset][:, None, :] * padded[:, offset : offset + tok_rows]
    gate_part = shorted[0]
    product = shorted[2] * shorted[1]
    spread = lax.all_to_all(product.T, "col", split_axis=0, concat_axis=1, tiled=True)
    first_channel = col_index * group_size
    own_rates = lax.dynamic_slice_in_dim(filter_decay, first_channel, group_size)
    mirror = lax.iota(jnp.int32, seq_len)
    hidden, tau_values = filter_hidden(mirror, seq_len, filter_first, filter_second)
    ahead_vals = side_values(
        hidden,
        tau_values,
        lax.dynamic_slice_in_dim(filter_ahead, first_channel, group_size, 1),
        own_rates,
    )
    behind_vals = side_values(
        hidden,
        tau_values,
        lax.dynamic_slice_in_dim(filter_behind, first_channel, group_size, 1),
        own_rates,
    )
    kernel = jnp.concatenate(
        [ahead_vals, jnp.zeros((group_size, 1), jnp.float32), jnp.flip(behind_vals[:, 1:], axis=1)],
        axis=1,
    )
    kernel = kernel * lax.rsqrt(jnp.sum(kernel * kernel, axis=1, keepdims=True) + 1e-06)
    factor = 128
    half_rows = factor // 2
    width_second = span_len // factor
    first_cos, first_sin = angle_table(factor, factor, factor)
    twist_cos, twist_sin = angle_table(factor, width_second, span_len)
    second_cos, second_sin = angle_table(width_second, width_second, width_second)
    first_table = jnp.stack([first_cos, -first_sin])
    last_table = jnp.stack([first_cos[:half_rows], -first_sin[:half_rows]], axis=1)
    twist_even = jnp.concatenate([twist_cos, twist_cos], axis=1)
    twist_ahead = jnp.concatenate([twist_sin, -twist_sin], axis=1)
    twist_back = jnp.concatenate([-twist_sin, twist_sin], axis=1)
    block_ahead = jnp.concatenate(
        [
            jnp.concatenate([second_cos, -second_sin], axis=1),
            jnp.concatenate([second_sin, second_cos], axis=1),
        ],
        axis=0,
    )
    block_back = jnp.concatenate(
        [
            jnp.concatenate([second_cos, second_sin], axis=1),
            jnp.concatenate([-second_sin, second_cos], axis=1),
        ],
        axis=0,
    )
    kernel_spec = forward(
        kernel.reshape(group_size, factor, width_second),
        first_table,
        twist_even,
        twist_ahead,
        block_ahead,
    )
    data_spec = forward(
        spread.reshape(group_size, half_rows, width_second),
        first_table[:, :, :half_rows],
        twist_even,
        twist_ahead,
        block_ahead,
    )
    data_re = data_spec[..., :width_second]
    data_im = data_spec[..., width_second:]
    kernel_re = kernel_spec[..., :width_second]
    kernel_im = kernel_spec[..., width_second:]
    joined = jnp.concatenate(
        [data_re * kernel_re - data_im * kernel_im, data_re * kernel_im + data_im * kernel_re],
        axis=-1,
    )
    convolved = inverse(joined, last_table, twist_even, twist_back, block_back, span_len).reshape(
        group_size, seq_len
    )
    returned = lax.all_to_all(convolved, "col", split_axis=1, concat_axis=0, tiled=True)
    mixed_rows = ((returned.T + skip_gain * product) * gate_part).astype(jnp.bfloat16)
    return jnp.dot(mixed_rows, out_weight, preferred_element_type=jnp.float32).astype(jnp.bfloat16)[
        None
    ]


f32, bf16 = (jnp.float32, jnp.bfloat16)
EDGE = 16
LANES = 128
FEATS = 64


def halves(table):
    high = table.astype(bf16)
    return [high, (table - high.astype(np.float64)).astype(bf16)]


def wave_tables(seq_len):
    odd = 2 * np.arange(seq_len, dtype=np.int64) + 1
    low = odd[: seq_len // 2]
    angle = (low[:, None] * odd[None, :] % (8 * seq_len)) * (math.pi / (4 * seq_len))
    table = np.concatenate([np.cos(angle), np.sin(angle)], axis=0)
    half = low * (math.pi / (4 * seq_len))
    turn = np.stack([np.cos(half), np.sin(half)]).astype(np.float32)
    turn = np.repeat(turn[:, :, None], LANES, axis=2)
    return (np.stack(halves(table)), np.stack(halves(table.T)), turn)


def feature_table(seq_len, feature_count):
    position = np.arange(seq_len, dtype=np.float64)
    bands = (feature_count - 1) // 2
    values = np.linspace(0.0001, bands - 1, bands)
    angles = (2.0 * math.pi / seq_len * position)[:, None] * values[None, :]
    tau = position / (seq_len - 1)
    table = np.concatenate([tau[:, None], np.cos(angles), -np.sin(angles)], axis=1)
    return np.concatenate(halves(np.pad(table, ((0, 0), (0, FEATS - feature_count)))), axis=1)


def sine(x):
    turns = jnp.floor(x * (1.0 / math.pi) + 0.5)
    r = x - turns * 3.140625
    r = r - turns * 9.67502593994140625e-4
    r = r - turns * 1.509957990978376432e-7
    sign = 1.0 - 2.0 * (turns - 2.0 * jnp.floor(turns * 0.5))
    s = r * r
    poly = 1.0 / 362880.0 - s * (1.0 / 39916800.0)
    poly = -1.0 / 5040.0 + s * poly
    poly = 1.0 / 120.0 + s * poly
    poly = -1.0 / 6.0 + s * poly
    return sign * (r + r * s * poly)


def split(value):
    high = value.astype(bf16)
    return (high, (value - high.astype(f32)).astype(bf16))


def mul(a, b):
    return jnp.dot(a, b, preferred_element_type=f32)


def joined(value, axis):
    return jnp.concatenate(split(value), axis=axis)


def twice(weight):
    both = joined(weight, 1)
    return jnp.concatenate([both, both], axis=0)


def neighbours(rows, before, after):
    count = rows.shape[0]
    index = lax.broadcasted_iota(jnp.int32, rows.shape, 0)
    up = jnp.where(index == 0, before, pltpu.roll(rows, 1, 0))
    down = jnp.where(index == count - 1, after, pltpu.roll(rows, count - 1, 0))
    return (up, down)


def short_form(rows, taps, before, after):
    up, down = neighbours(rows, before, after)
    return taps[0:1] * up + taps[1:2] * rows + taps[2:3] * down


def conv_kernel(
    n,
    gate_hbm,
    mult_hbm,
    value_hbm,
    taps_gate_hbm,
    taps_mult_hbm,
    taps_value_hbm,
    first_hbm,
    second_hbm,
    ahead_hbm,
    behind_hbm,
    decay_hbm,
    skip_hbm,
    weight_hbm,
    table_hbm,
    table_t_hbm,
    turn_hbm,
    feature_hbm,
    out_ref,
    rims,
    gate,
    mult,
    value,
    taps_gate,
    taps_mult,
    taps_value,
    second_ref,
    decay_ref,
    skip_ref,
    first,
    ahead_w,
    behind_w,
    weight,
    table,
    table_t,
    turn,
    feature,
    halo_sent,
    halo_came,
    sent,
    came,
    wide_sent,
    rim_sent,
    wide_came,
    back_sent,
    back_came,
    near_sent,
    near_came,
    kernel_re,
    kernel_im,
    spec,
    gate_part,
    direct,
    total,
    load_sems,
    send_sems,
    recv_sems,
    wide_send,
    wide_recv,
    back_send,
    back_recv,
    near_sems,
    halo_send,
    halo_recv,
):
    me = lax.axis_index("col")
    rows, channels = gate.shape
    slabs = channels // LANES
    share = (slabs - n) // 2
    seq_len = rows * n
    half = seq_len // 2
    core = lax.rem(me, 2)
    near = me + 1 - 2 * core
    far = []
    for j in range(1, n // 2):
        chip = lax.rem(me - core + 2 * j, n)
        far += [chip, chip + 1]
    peers = far + [near]

    barrier = pltpu.get_barrier_semaphore()
    for peer in peers:
        pl.semaphore_signal(
            barrier, inc=1, device_id={"col": peer}, device_id_type=pl.DeviceIdType.MESH
        )

    def lanes(slab, count=1):
        start = slab * LANES
        if not isinstance(slab, int):
            start = pl.multiple_of(start, LANES)
        return pl.ds(start, count * LANES)

    def span(owner):
        return pl.ds(pl.multiple_of(owner * rows, rows), rows)

    loads = {}

    def load(name, src, dst):
        copy = pltpu.make_async_copy(src, dst, load_sems.at[len(loads)])
        copy.start()
        loads[name] = copy

    def ready(*names):
        for name in names:
            loads[name].wait()

    def remote(src, dst, ssem, rsem, peer):
        return pltpu.make_async_remote_copy(
            src_ref=src,
            dst_ref=dst,
            send_sem=ssem,
            recv_sem=rsem,
            device_id={"col": peer},
            device_id_type=pl.DeviceIdType.MESH,
        )

    for side, base in enumerate((rows - EDGE, 0)):
        for i, ref in enumerate((gate_hbm, mult_hbm, value_hbm)):
            load(f"rim{side}{i}", ref.at[0, pl.ds(base, EDGE)], rims.at[side, i])
    load("taps_value", taps_value_hbm, taps_value)
    load("taps_mult", taps_mult_hbm, taps_mult)
    for i, (low, count) in enumerate(((0, n), (n, slabs - n))):
        load(f"value{i}", value_hbm.at[0, :, lanes(low, count)], value.at[:, lanes(low, count)])
        load(f"mult{i}", mult_hbm.at[0, :, lanes(low, count)], mult.at[:, lanes(low, count)])
    own_wide = n + share * core
    load("feature", feature_hbm, feature)
    load("first", first_hbm, first.at[pl.ds(0, first_hbm.shape[0])])
    load("second", second_hbm, second_ref)
    load("decay", decay_hbm, decay_ref)
    for name, s, d in (("ahead", ahead_hbm, ahead_w), ("behind", behind_hbm, behind_w)):
        load(name + "0", s.at[:, lanes(me)], d.at[:, lanes(0)])
        load(name + "1", s.at[:, lanes(own_wide, share)], d.at[:, lanes(1, share)])

    copies = []

    def send(*args):
        copy = remote(*args)
        copy.start()
        copies.append(copy)

    ready(*(f"rim{side}{i}" for side in range(2) for i in range(3)))
    right, left = (lax.rem(me + 1, n), lax.rem(me + n - 1, n))
    for side, at in enumerate((EDGE - 1, 0)):
        parts = []
        for i in range(3):
            line = rims[side, i].astype(f32)[at : at + 1]
            parts.append(
                jnp.concatenate([line[:, b * LANES : (b + 1) * LANES] for b in range(slabs)], axis=0)
            )
        halo_sent[side] = jnp.concatenate(parts, axis=1).astype(bf16)
    pl.semaphore_wait(barrier, n - 1)
    for side, target in enumerate((right, left)):
        send(
            halo_sent.at[side], halo_came.at[side], halo_send.at[side], halo_recv.at[side], target
        )

    zero = jnp.zeros((1, LANES), f32)

    def short_product(v, m, slab):
        vs = short_form(v, taps_value[:, lanes(slab)], zero, zero)
        ms = short_form(m, taps_mult[:, lanes(slab)], zero, zero)
        return (vs * ms).astype(bf16)

    def pack(owner):
        v = value[:, lanes(owner)].astype(f32)
        m = mult[:, lanes(owner)].astype(f32)
        sent[owner, pl.ds(0, rows), :] = short_product(v, m, owner)
        edges = [v[0:2], v[rows - 2 : rows], m[0:2], m[rows - 2 : rows], jnp.zeros((8, LANES), f32)]
        sent[owner, pl.ds(rows, EDGE), :] = jnp.concatenate(edges, axis=0).astype(bf16)

    ready("taps_value", "taps_mult", "value0", "mult0")
    for peer in peers:
        pack(peer)
        send(sent.at[peer], came.at[me], send_sems.at[peer], recv_sems.at[me], peer)
    pack(me)

    ready("value1", "mult1")
    for slab in range(n, slabs):
        cols = lanes(slab)
        wide_sent[slab - n] = short_product(value[:, cols].astype(f32), mult[:, cols].astype(f32), slab)
    inner = pl.ds(EDGE, rows - 2 * EDGE)

    def inner_of(owner):
        return pl.ds(pl.multiple_of(owner * rows + EDGE, EDGE), rows - 2 * EDGE)

    def rim_of(owner, side):
        return pl.ds(pl.multiple_of(owner * rows + (1 - side) * (rows - EDGE), EDGE), EDGE)

    def own_share(peer):
        return pl.ds(lax.rem(peer, 2) * share, share)

    for peer in peers:
        send(
            wide_sent.at[own_share(peer), inner],
            wide_came.at[:, inner_of(me)],
            wide_send.at[0, peer],
            wide_recv.at[0, me],
            peer,
        )
    for j in range(share):
        wide_came[j, inner_of(me), :] = wide_sent[core * share + j, inner, :]

    load("table", table_hbm, table)
    load("turn", turn_hbm, turn)
    load("table_t", table_t_hbm, table_t)
    load("gate", gate_hbm.at[0], gate)
    load("taps_gate", taps_gate_hbm, taps_gate)
    load("skip", skip_hbm, skip_ref)
    load("weight", weight_hbm, weight)

    def signs(shape):
        return (1 - 2 * (lax.broadcasted_iota(jnp.int32, shape, 0) % 2)).astype(f32)

    ready("feature", "first", "second")
    used = first_hbm.shape[0]
    at = lax.broadcasted_iota(jnp.int32, first.shape, 0)
    wide = mul(feature[...], twice(jnp.where(at < used, first[...], 0.0)))
    hidden = sine(wide[:, :LANES] + wide[:, LANES:])
    wide = mul(joined(hidden, 1), twice(second_ref[...]))
    hidden = sine(wide[:, :LANES] + wide[:, LANES:])
    row_at = lax.broadcasted_iota(jnp.int32, hidden.shape, 0)
    later = jnp.where(row_at == seq_len - 1, 0.0, pltpu.roll(hidden, seq_len - 1, 0))
    ready("decay", "ahead0", "ahead1", "behind0", "behind1")
    both_rates = [decay_ref[:, lanes(me)], decay_ref[:, lanes(own_wide, share)]]
    rates = jnp.concatenate(both_rates, axis=1) * (-1.0 / (seq_len - 1))
    index = lax.broadcasted_iota(jnp.int32, (seq_len, (1 + share) * LANES), 0)
    fade = jnp.exp(rates * index.astype(f32))

    def side_of(values, w):
        high, low = split(w)
        return mul(values, jnp.concatenate([high, high], axis=0)) + mul(
            values, jnp.concatenate([low, low], axis=0)
        )

    ahead = side_of(joined(hidden, 1), ahead_w[...])
    behind = side_of(joined(later, 1), behind_w[...] * jnp.exp(rates))
    sums = (ahead + behind) * fade
    gaps = (ahead - behind) * fade
    power = jnp.sum(sums * sums + gaps * gaps, axis=0, keepdims=True) * 0.5
    scale = lax.rsqrt(power + 1e-06) * (2.0 / (2 * seq_len))
    flip = signs((seq_len, LANES)).astype(bf16)
    ready("table", "turn")
    cos_half = turn[0][:, 0:1]
    sin_half = turn[1][:, 0:1]
    for j in range(1 + share):
        cols = slice(j * LANES, (j + 1) * LANES)
        sh, sl = split(sums[:, cols])
        gh, gl = split(gaps[:, cols])

        def turned(rows_at, a, b):
            high = jnp.concatenate([a[0], b[0] * flip], axis=1)
            low = jnp.concatenate([a[1], b[1] * flip], axis=1)
            t0 = table[0, rows_at : rows_at + half, :]
            t1 = table[1, rows_at : rows_at + half, :]
            return mul(t0, high) + mul(t1, high) + mul(t0, low)

        top = turned(0, (sh, sl), (gh, gl))
        bottom = turned(half, (gh, gl), (sh, sl))
        kernel_re[j] = cos_half * top + sin_half * bottom
        kernel_im[j] = sin_half * top - cos_half * bottom

    for side, target in enumerate((right, left)):
        remote(
            halo_sent.at[side], halo_came.at[side], halo_send.at[side], halo_recv.at[side], target
        ).wait_recv()
    befores = halo_came[0].astype(f32) * (me > 0).astype(f32)
    afters = halo_came[1].astype(f32) * (me < n - 1).astype(f32)

    def line_of(halo, i, slab):
        return halo[slab : slab + 1, i * LANES : (i + 1) * LANES]

    rim_at = lax.broadcasted_iota(jnp.int32, (EDGE, LANES), 0)
    for slab in range(n, slabs):
        first_row = last_row = 1.0
        for i, taps in ((1, taps_mult), (2, taps_value)):
            t = taps[:, lanes(slab)]
            upper = rims[1, i, :, lanes(slab)].astype(f32)
            lower = rims[0, i, :, lanes(slab)].astype(f32)
            first_row *= (
                t[0:1] * line_of(befores, i, slab) + t[1:2] * upper[0:1] + t[2:3] * upper[1:2]
            )
            last_row *= (
                t[0:1] * lower[EDGE - 2 : EDGE - 1]
                + t[1:2] * lower[EDGE - 1 : EDGE]
                + t[2:3] * line_of(afters, i, slab)
            )
        for side, row, where in ((1, first_row, 0), (0, last_row, EDGE - 1)):
            base = 0 if side else rows - EDGE
            old = wide_sent[slab - n, base : base + EDGE, :].astype(f32)
            rim_sent[side, slab - n] = jnp.where(rim_at == where, row, old).astype(bf16)
    for peer in peers:
        for side in range(2):
            send(
                rim_sent.at[side, own_share(peer)],
                wide_came.at[:, rim_of(me, side)],
                wide_send.at[1 + side, peer],
                wide_recv.at[1 + side, me],
                peer,
            )
    for j in range(share):
        for side in range(2):
            wide_came[j, rim_of(me, side), :] = rim_sent[side, core * share + j]

    alternate = signs((rows, LANES))

    def convolve(j, x):
        freq = mul(table[0], jnp.concatenate([x, x * flip], axis=1))
        top, bottom = (freq[:half], freq[half:])
        kr, ki = (kernel_re[j], kernel_im[j])
        spec[j, :half] = (top * kr + bottom * ki).astype(bf16)
        spec[j, half:] = (bottom * kr - top * ki).astype(bf16)

    def invert(owner, j):
        both = mul(table_t[0, span(owner), :], spec[j])
        back = both[:, :LANES] + alternate * both[:, LANES:]
        return back * scale[:, j * LANES : (j + 1) * LANES]

    came[me] = sent[me]
    for peer in reversed(peers):
        remote(
            sent.at[peer], came.at[peer], send_sems.at[peer], recv_sems.at[peer], peer
        ).wait_recv()
    edges = [came[s, pl.ds(rows, EDGE), :].astype(f32) for s in range(n)]
    own_taps = [t[:, lanes(me)] for t in (taps_value, taps_mult)]
    pieces = []
    for s in range(n):
        top = bottom = 1.0
        for k, taps in enumerate(own_taps):
            e = edges[s][4 * k : 4 * k + 4]
            first_row = taps[1:2] * e[0:1] + taps[2:3] * e[1:2]
            last_row = taps[0:1] * e[2:3] + taps[1:2] * e[3:4]
            if s > 0:
                first_row += taps[0:1] * edges[s - 1][4 * k + 3 : 4 * k + 4]
            if s < n - 1:
                last_row += taps[2:3] * edges[s + 1][4 * k : 4 * k + 1]
            top, bottom = (top * first_row, bottom * last_row)
        block = came[s, pl.ds(0, rows), :]
        upper = jnp.where(rim_at == 0, top, block[:EDGE].astype(f32)).astype(bf16)
        lower = jnp.where(rim_at == EDGE - 1, bottom, block[rows - EDGE :].astype(f32)).astype(bf16)
        pieces += [upper, block[EDGE : rows - EDGE], lower]
    ready("table_t")
    convolve(0, jnp.concatenate(pieces, axis=0))
    for peer in peers:
        back_sent[peer] = invert(peer, 0).astype(bf16)
        send(back_sent.at[peer], back_came.at[me], back_send.at[peer], back_recv.at[me], peer)
    own_back = invert(me, 0)

    ready("gate", "taps_gate", "skip")
    for slab in range(slabs):
        cols = lanes(slab)
        parts = []
        for i, (r, taps) in enumerate(((gate, taps_gate), (mult, taps_mult), (value, taps_value))):
            parts.append(
                short_form(
                    r[:, cols].astype(f32), taps[:, cols], line_of(befores, i, slab), line_of(afters, i, slab)
                )
            )
        gate_part[slab] = parts[0]
        direct[slab] = skip_ref[:, cols] * (parts[1] * parts[2])
    ready("weight")

    def gated(slab, convolved):
        return ((convolved + direct[slab]) * gate_part[slab]).astype(bf16)

    def project(items):
        left_side = jnp.concatenate([gated(slab, value) for slab, value in items], axis=1)
        return mul(left_side, jnp.concatenate([weight[lanes(slab), :] for slab, _ in items], axis=0))

    def returned(peer):
        remote(
            back_sent.at[peer], back_came.at[peer], back_send.at[peer], back_recv.at[peer], peer
        ).wait_recv()
        return (peer, back_came[peer].astype(f32))

    for peer in reversed(peers):
        for i in range(3):
            where = inner_of(peer) if i == 0 else rim_of(peer, i - 1)
            what = wide_sent.at[own_share(me), inner] if i == 0 else rim_sent.at[i - 1, own_share(me)]
            remote(
                what, wide_came.at[:, where], wide_send.at[i, peer], wide_recv.at[i, peer], peer
            ).wait_recv()
    for j in range(share):
        convolve(1 + j, wide_came[j])
    for j in range(share):
        near_sent[j] = invert(near, 1 + j).astype(bf16)
    send(near_sent, near_came, near_sems.at[0], near_sems.at[1], near)
    items = [(own_wide + j, invert(me, 1 + j)) for j in range(share)]
    items += [(me, own_back), returned(near)]
    total[...] = project(items)
    items = [returned(peer) for peer in reversed(far)]
    remote(near_sent, near_came, near_sems.at[0], near_sems.at[1], near).wait_recv()
    near_wide = n + share * (1 - core)
    items += [(near_wide + j, near_came[j].astype(f32)) for j in range(share)]
    out_ref[0] = (total[...] + project(items)).astype(bf16)
    for copy in copies:
        copy.wait_send()


def fused_body(n, *args):
    gate_in, mult_in, value_in, tg, tm, tv, first, second, ahead, behind, decay, skip, weight = args
    _, rows, channels = gate_in.shape
    seq_len = rows * n
    half = seq_len // 2
    width = weight.shape[1]
    slabs = channels // LANES
    share = (slabs - n) // 2
    table, table_t, turn = wave_tables(seq_len)
    table_t = table_t[:1]
    features = feature_table(seq_len, first.shape[0])
    vmem = pl.BlockSpec(memory_space=pltpu.VMEM)
    main = pl.BlockSpec(memory_space=pltpu.HBM)
    hidden_count = second.shape[0]
    dma = pltpu.SemaphoreType.DMA
    return pl.pallas_call(
        functools.partial(conv_kernel, n),
        out_shape=pltpu.VMEM((1, rows, width), bf16),
        in_specs=[main] * 17,
        out_specs=vmem,
        scratch_shapes=[
            pltpu.VMEM((2, 3, EDGE, channels), bf16),
            pltpu.VMEM((rows, channels), bf16),
            pltpu.VMEM((rows, channels), bf16),
            pltpu.VMEM((rows, channels), bf16),
            pltpu.VMEM(tg.shape, f32),
            pltpu.VMEM(tm.shape, f32),
            pltpu.VMEM(tv.shape, f32),
            pltpu.VMEM(second.shape, f32),
            pltpu.VMEM((1, channels), f32),
            pltpu.VMEM((1, channels), f32),
            pltpu.VMEM((FEATS, hidden_count), f32),
            pltpu.VMEM((hidden_count, (1 + share) * LANES), f32),
            pltpu.VMEM((hidden_count, (1 + share) * LANES), f32),
            pltpu.VMEM(weight.shape, bf16),
            pltpu.VMEM(table.shape, bf16),
            pltpu.VMEM(table_t.shape, bf16),
            pltpu.VMEM(turn.shape, f32),
            pltpu.VMEM(features.shape, bf16),
            pltpu.VMEM((2, slabs, 3 * LANES), bf16),
            pltpu.VMEM((2, slabs, 3 * LANES), bf16),
            pltpu.VMEM((n, rows + EDGE, LANES), bf16),
            pltpu.VMEM((n, rows + EDGE, LANES), bf16),
            pltpu.VMEM((2 * share, rows, LANES), bf16),
            pltpu.VMEM((2, 2 * share, EDGE, LANES), bf16),
            pltpu.VMEM((share, seq_len, LANES), bf16),
            pltpu.VMEM((n, rows, LANES), bf16),
            pltpu.VMEM((n, rows, LANES), bf16),
            pltpu.VMEM((share, rows, LANES), bf16),
            pltpu.VMEM((share, rows, LANES), bf16),
            pltpu.VMEM((1 + share, half, 2 * LANES), f32),
            pltpu.VMEM((1 + share, half, 2 * LANES), f32),
            pltpu.VMEM((1 + share, seq_len, 2 * LANES), bf16),
            pltpu.VMEM((slabs, rows, LANES), f32),
            pltpu.VMEM((slabs, rows, LANES), f32),
            pltpu.VMEM((rows, width), f32),
            dma((32,)),
            dma((n,)),
            dma((n,)),
            dma((3, n)),
            dma((3, n)),
            dma((n,)),
            dma((n,)),
            dma((2,)),
            dma((2,)),
            dma((2,)),
        ],
        compiler_params=pltpu.CompilerParams(
            collective_id=0, has_side_effects=True, vmem_limit_bytes=61 * 1024 * 1024
        ),
    )(
        gate_in, mult_in, value_in, tg, tm, tv, first, second, ahead, behind,
        decay.reshape(1, channels), skip.reshape(1, channels), weight,
        jnp.asarray(table), jnp.asarray(table_t), jnp.asarray(turn), jnp.asarray(features),
    )


def body_for(n, *args):
    _, rows, channels = args[0].shape
    small = rows * n <= 1024 and rows % 128 == 0 and channels % (2 * LANES) == 0
    spare = channels // LANES > n
    network = args[6].shape[0] <= FEATS and args[6].shape[1] == 128
    if n >= 2 and n % 2 == 0 and small and spare and network and args[3].shape[0] == 3:
        return fused_body(n, *args)
    return spread_body(*args)


def solution(mesh):
    in_specs = (
        P(("grp", "row"), "col", None),
        P(("grp", "row"), "col", None),
        P(("grp", "row"), "col", None),
        P(),
        P(),
        P(),
        P(),
        P(),
        P(),
        P(),
        P(),
        P(),
        P(),
    )
    out_specs = P(("grp", "row"), "col", None)

    body = functools.partial(body_for, mesh.shape["col"])
    return jax.shard_map(body, mesh=mesh, in_specs=in_specs, out_specs=out_specs, check_vma=False)
```

```python
import functools
import math

import jax
import jax.numpy as jnp
import numpy as np
from jax import lax
from jax.experimental import pallas as pl
from jax.experimental.pallas import tpu as pltpu
from jax.sharding import PartitionSpec as P

highest = lax.Precision.HIGHEST


def padded_2(shard, sides, width):
    for axis, dim in sides:
        size, length = (lax.axis_size(axis), shard.shape[dim])
        up = [(i, (i + 1) % size) for i in range(size - 1)]
        down = [(j, i) for i, j in up]
        last = lax.slice_in_dim(shard, length - width, length, axis=dim)
        leading = lax.slice_in_dim(shard, 0, width, axis=dim)
        before = lax.ppermute(last, axis, up)
        after = lax.ppermute(leading, axis, down)
        shard = jnp.concatenate([before, shard, after], axis=dim)
    return shard


def filter_hidden(mirror, seq_len, filter_first, filter_second):
    tau_values = mirror.astype(jnp.float32) / (seq_len - 1)
    omega_pos = 2.0 * math.pi / seq_len * mirror.astype(jnp.float32)
    band_count = (filter_first.shape[0] - 1) // 2
    band_values = jnp.linspace(0.0001, band_count - 1, band_count, dtype=jnp.float32)
    angles = omega_pos[:, None] * band_values[None, :]
    features = jnp.concatenate([tau_values[:, None], jnp.cos(angles), -jnp.sin(angles)], axis=1)
    hidden = jnp.sin(jnp.dot(features, filter_first, precision=highest))
    hidden = jnp.sin(jnp.dot(hidden, filter_second, precision=highest))
    return (hidden, tau_values)


def side_values(hidden, tau_values, side_weight, decay_rates):
    values = jnp.einsum("pf,fh->hp", hidden, side_weight, precision=highest)
    return values * jnp.exp(-decay_rates[:, None] * tau_values[None, :])


def angle_table(row_count, column_count, period):
    products = (
        lax.iota(jnp.int32, row_count)[:, None]
        * lax.iota(jnp.int32, column_count)[None, :]
        % period
    )
    angle = products.astype(jnp.float32) * (2.0 * math.pi / period)
    return (jnp.cos(angle), jnp.sin(angle))


def swap_halves(stacked, width):
    return jnp.concatenate([stacked[..., width:], stacked[..., :width]], axis=-1)


def forward(values, first_table, twist_even, twist_odd, second_block):
    channels, _, width = values.shape
    first = jnp.einsum("sfa,cab->cfsb", first_table, values, precision=highest)
    first = first.reshape(channels, first_table.shape[1], 2 * width)
    turned = first * twist_even + swap_halves(first, width) * twist_odd
    return jnp.einsum("cfk,kl->cfl", turned, second_block, precision=highest)


def inverse(spectrum, last_table, twist_even, twist_odd, second_block, span_len):
    channels, freq_rows, double_width = spectrum.shape
    width = double_width // 2
    back = jnp.einsum("cfk,kl->cfl", spectrum, second_block, precision=highest)
    turned = back * twist_even + swap_halves(back, width) * twist_odd
    turned = turned.reshape(channels, freq_rows, 2, width)
    result = jnp.einsum("asf,cfsb->cab", last_table, turned, precision=highest)
    return result / span_len


def spread_body(
    gate_in,
    mult_in,
    value_in,
    taps_gate,
    taps_mult,
    taps_value,
    filter_first,
    filter_second,
    filter_ahead,
    filter_behind,
    filter_decay,
    skip_gain,
    out_weight,
):
    col_count = lax.axis_size("col")
    col_index = lax.axis_index("col")
    tok_rows = gate_in.shape[1]
    seq_len = tok_rows * col_count
    span_len = 2 * seq_len
    group_size = filter_ahead.shape[1] // col_count
    stacked = jnp.stack([gate_in[0], mult_in[0], value_in[0]])
    padded = padded_2(stacked, (("col", 1),), 1).astype(jnp.float32)
    all_taps = jnp.stack([taps_gate, taps_mult, taps_value])
    shorted = jnp.zeros(stacked.shape, jnp.float32)
    for offset in range(all_taps.shape[1]):
        shorted = shorted + all_taps[:, offset][:, None, :] * padded[:, offset : offset + tok_rows]
    gate_part = shorted[0]
    product = shorted[2] * shorted[1]
    spread = lax.all_to_all(product.T, "col", split_axis=0, concat_axis=1, tiled=True)
    first_channel = col_index * group_size
    own_rates = lax.dynamic_slice_in_dim(filter_decay, first_channel, group_size)
    mirror = lax.iota(jnp.int32, seq_len)
    hidden, tau_values = filter_hidden(mirror, seq_len, filter_first, filter_second)
    ahead_vals = side_values(
        hidden,
        tau_values,
        lax.dynamic_slice_in_dim(filter_ahead, first_channel, group_size, 1),
        own_rates,
    )
    behind_vals = side_values(
        hidden,
        tau_values,
        lax.dynamic_slice_in_dim(filter_behind, first_channel, group_size, 1),
        own_rates,
    )
    kernel = jnp.concatenate(
        [ahead_vals, jnp.zeros((group_size, 1), jnp.float32), jnp.flip(behind_vals[:, 1:], axis=1)],
        axis=1,
    )
    kernel = kernel * lax.rsqrt(jnp.sum(kernel * kernel, axis=1, keepdims=True) + 1e-06)
    factor = 128
    half_rows = factor // 2
    width_second = span_len // factor
    first_cos, first_sin = angle_table(factor, factor, factor)
    twist_cos, twist_sin = angle_table(factor, width_second, span_len)
    second_cos, second_sin = angle_table(width_second, width_second, width_second)
    first_table = jnp.stack([first_cos, -first_sin])
    last_table = jnp.stack([first_cos[:half_rows], -first_sin[:half_rows]], axis=1)
    twist_even = jnp.concatenate([twist_cos, twist_cos], axis=1)
    twist_ahead = jnp.concatenate([twist_sin, -twist_sin], axis=1)
    twist_back = jnp.concatenate([-twist_sin, twist_sin], axis=1)
    block_ahead = jnp.concatenate(
        [
            jnp.concatenate([second_cos, -second_sin], axis=1),
            jnp.concatenate([second_sin, second_cos], axis=1),
        ],
        axis=0,
    )
    block_back = jnp.concatenate(
        [
            jnp.concatenate([second_cos, second_sin], axis=1),
            jnp.concatenate([-second_sin, second_cos], axis=1),
        ],
        axis=0,
    )
    kernel_spec = forward(
        kernel.reshape(group_size, factor, width_second),
        first_table,
        twist_even,
        twist_ahead,
        block_ahead,
    )
    data_spec = forward(
        spread.reshape(group_size, half_rows, width_second),
        first_table[:, :, :half_rows],
        twist_even,
        twist_ahead,
        block_ahead,
    )
    data_re = data_spec[..., :width_second]
    data_im = data_spec[..., width_second:]
    kernel_re = kernel_spec[..., :width_second]
    kernel_im = kernel_spec[..., width_second:]
    joined = jnp.concatenate(
        [data_re * kernel_re - data_im * kernel_im, data_re * kernel_im + data_im * kernel_re],
        axis=-1,
    )
    convolved = inverse(joined, last_table, twist_even, twist_back, block_back, span_len).reshape(
        group_size, seq_len
    )
    returned = lax.all_to_all(convolved, "col", split_axis=1, concat_axis=0, tiled=True)
    mixed_rows = ((returned.T + skip_gain * product) * gate_part).astype(jnp.bfloat16)
    return jnp.dot(mixed_rows, out_weight, preferred_element_type=jnp.float32).astype(jnp.bfloat16)[
        None
    ]


f32, bf16 = (jnp.float32, jnp.bfloat16)
EDGE = 16
ENDS = 8
LANES = 128
FEATS = 64


def halves(table):
    high = table.astype(bf16)
    return [high, (table - high.astype(np.float64)).astype(bf16)]


def wave_tables(seq_len):
    odd = 2 * np.arange(seq_len, dtype=np.int64) + 1
    low = odd[: seq_len // 2]
    angle = (low[:, None] * odd[None, :] % (8 * seq_len)) * (math.pi / (4 * seq_len))
    table = np.concatenate([np.cos(angle), np.sin(angle)], axis=0)
    half = low * (math.pi / (4 * seq_len))
    turn = np.stack([np.cos(half), np.sin(half)]).astype(np.float32)
    turn = np.repeat(turn[:, :, None], LANES, axis=2)
    return (np.stack(halves(table)), np.stack(halves(table.T)), turn)


def feature_table(seq_len, feature_count):
    position = np.arange(seq_len, dtype=np.float64)
    bands = (feature_count - 1) // 2
    values = np.linspace(0.0001, bands - 1, bands)
    angles = (2.0 * math.pi / seq_len * position)[:, None] * values[None, :]
    tau = position / (seq_len - 1)
    table = np.concatenate([tau[:, None], np.cos(angles), -np.sin(angles)], axis=1)
    return np.concatenate(halves(np.pad(table, ((0, 0), (0, FEATS - feature_count)))), axis=1)


def sine(x):
    turns = jnp.floor(x * (1.0 / math.pi) + 0.5)
    r = x - turns * 3.140625
    r = r - turns * 9.67502593994140625e-4
    r = r - turns * 1.509957990978376432e-7
    sign = 1.0 - 2.0 * (turns - 2.0 * jnp.floor(turns * 0.5))
    s = r * r
    poly = 1.0 / 362880.0 - s * (1.0 / 39916800.0)
    poly = -1.0 / 5040.0 + s * poly
    poly = 1.0 / 120.0 + s * poly
    poly = -1.0 / 6.0 + s * poly
    return sign * (r + r * s * poly)


def split(value):
    high = value.astype(bf16)
    return (high, (value - high.astype(f32)).astype(bf16))


def mul(a, b):
    return jnp.dot(a, b, preferred_element_type=f32)


def joined(value, axis):
    return jnp.concatenate(split(value), axis=axis)


def twice(weight):
    both = joined(weight, 1)
    return jnp.concatenate([both, both], axis=0)


def neighbours(rows, before, after):
    count = rows.shape[0]
    index = lax.broadcasted_iota(jnp.int32, rows.shape, 0)
    up = jnp.where(index == 0, before, pltpu.roll(rows, 1, 0))
    down = jnp.where(index == count - 1, after, pltpu.roll(rows, count - 1, 0))
    return (up, down)


def short_form(rows, taps, before, after):
    up, down = neighbours(rows, before, after)
    return taps[0:1] * up + taps[1:2] * rows + taps[2:3] * down


def conv_kernel(
    n,
    gate_hbm,
    mult_hbm,
    value_hbm,
    taps_gate_hbm,
    taps_mult_hbm,
    taps_value_hbm,
    first_hbm,
    second_hbm,
    ahead_hbm,
    behind_hbm,
    decay_hbm,
    skip_hbm,
    weight_hbm,
    table_hbm,
    table_t_hbm,
    turn_hbm,
    feature_hbm,
    out_ref,
    rims,
    gate,
    mult,
    value,
    taps_gate,
    taps_mult,
    taps_value,
    second_ref,
    decay_ref,
    skip_ref,
    first,
    ahead_w,
    behind_w,
    weight,
    table,
    table_t,
    turn,
    feature,
    halo_sent,
    halo_came,
    sent,
    came,
    wide_sent,
    rim_sent,
    wide_came,
    back_sent,
    back_came,
    near_sent,
    near_came,
    kernel_re,
    kernel_im,
    spec,
    gate_part,
    direct,
    total,
    partial,
    load_sems,
    send_sems,
    recv_sems,
    wide_send,
    wide_recv,
    back_send,
    back_recv,
    near_send,
    near_recv,
    halo_send,
    halo_recv,
):
    me = lax.axis_index("col")
    rows, channels = gate.shape
    slabs = channels // LANES
    share = (slabs - n) // 2
    seq_len = rows * n
    half = seq_len // 2
    core = lax.rem(me, 2)
    near = me + 1 - 2 * core
    far = []
    for j in range(1, n // 2):
        chip = lax.rem(me - core + 2 * j, n)
        far += [chip, chip + 1]
    peers = far + [near]

    halo_came[...] = jnp.zeros_like(halo_came)
    barrier = pltpu.get_barrier_semaphore()
    for peer in peers:
        pl.semaphore_signal(
            barrier, inc=1, device_id={"col": peer}, device_id_type=pl.DeviceIdType.MESH
        )

    def lanes(slab, count=1):
        start = slab * LANES
        if not isinstance(slab, int):
            start = pl.multiple_of(start, LANES)
        return pl.ds(start, count * LANES)

    def span(owner):
        return pl.ds(pl.multiple_of(owner * rows, rows), rows)

    loads = {}

    def load(name, src, dst):
        copy = pltpu.make_async_copy(src, dst, load_sems.at[len(loads)])
        copy.start()
        loads[name] = copy

    def ready(*names):
        for name in names:
            loads[name].wait()

    def remote(src, dst, ssem, rsem, peer):
        return pltpu.make_async_remote_copy(
            src_ref=src,
            dst_ref=dst,
            send_sem=ssem,
            recv_sem=rsem,
            device_id={"col": peer},
            device_id_type=pl.DeviceIdType.MESH,
        )

    for side, base in enumerate((rows - EDGE, 0)):
        for i, ref in enumerate((gate_hbm, mult_hbm, value_hbm)):
            load(f"rim{side}{i}", ref.at[0, pl.ds(base, EDGE)], rims.at[side, i])
    load("taps_value", taps_value_hbm, taps_value)
    load("taps_mult", taps_mult_hbm, taps_mult)
    for i, (low, count) in enumerate(((0, n), (n, slabs - n))):
        load(f"value{i}", value_hbm.at[0, :, lanes(low, count)], value.at[:, lanes(low, count)])
        load(f"mult{i}", mult_hbm.at[0, :, lanes(low, count)], mult.at[:, lanes(low, count)])
    own_wide = n + share * core
    load("feature", feature_hbm, feature)
    load("first", first_hbm, first.at[pl.ds(0, first_hbm.shape[0])])
    load("second", second_hbm, second_ref)
    load("decay", decay_hbm, decay_ref)
    for name, s, d in (("ahead", ahead_hbm, ahead_w), ("behind", behind_hbm, behind_w)):
        load(name + "0", s.at[:, lanes(me)], d.at[:, lanes(0)])
        load(name + "1", s.at[:, lanes(own_wide, share)], d.at[:, lanes(1, share)])

    copies = []

    def send(*args):
        copy = remote(*args)
        copy.start()
        copies.append(copy)

    ready(*(f"rim{side}{i}" for side in range(2) for i in range(3)))
    right, left = (lax.rem(me + 1, n), lax.rem(me + n - 1, n))
    for side, at in enumerate((EDGE - 1, 0)):
        parts = []
        for i in range(3):
            line = rims[side, i].astype(f32)[at : at + 1]
            parts.append(
                jnp.concatenate([line[:, b * LANES : (b + 1) * LANES] for b in range(slabs)], axis=0)
            )
        halo_sent[side] = jnp.concatenate(parts, axis=1).astype(bf16)
    pl.semaphore_wait(barrier, n - 1)

    def halo(side):
        return remote(
            halo_sent.at[side],
            halo_came.at[side],
            halo_send.at[side],
            halo_recv.at[side],
            (right, left)[side],
        )

    inside = (me < n - 1, me > 0)
    for side in range(2):
        pl.when(inside[side])(halo(side).start)

    zero = jnp.zeros((1, LANES), f32)

    def short_product(v, m, slab):
        vs = short_form(v, taps_value[:, lanes(slab)], zero, zero)
        ms = short_form(m, taps_mult[:, lanes(slab)], zero, zero)
        return (vs * ms).astype(bf16)

    def pack(owner):
        v = value[:, lanes(owner)].astype(f32)
        m = mult[:, lanes(owner)].astype(f32)
        sent[owner, pl.ds(0, rows), :] = short_product(v, m, owner)
        edges = [v[0:2], v[rows - 2 : rows], m[0:2], m[rows - 2 : rows]]
        sent[owner, pl.ds(rows, ENDS), :] = jnp.concatenate(edges, axis=0).astype(bf16)

    ready("taps_value", "taps_mult", "value0", "mult0")
    for peer in peers:
        pack(peer)
        send(sent.at[peer], came.at[me], send_sems.at[peer], recv_sems.at[me], peer)
    pack(me)

    ready("value1", "mult1")
    for slab in range(n, slabs):
        cols = lanes(slab)
        wide_sent[slab - n] = short_product(value[:, cols].astype(f32), mult[:, cols].astype(f32), slab)
    inner = pl.ds(EDGE, rows - 2 * EDGE)

    def inner_of(owner):
        return pl.ds(pl.multiple_of(owner * rows + EDGE, EDGE), rows - 2 * EDGE)

    def rim_of(owner, side):
        return pl.ds(pl.multiple_of(owner * rows + (1 - side) * (rows - EDGE), EDGE), EDGE)

    def own_share(peer):
        return pl.ds(lax.rem(peer, 2) * share, share)

    for peer in peers:
        send(
            wide_sent.at[own_share(peer), inner],
            wide_came.at[:, inner_of(me)],
            wide_send.at[0, peer],
            wide_recv.at[0, me],
            peer,
        )
    for j in range(share):
        wide_came[j, inner_of(me), :] = wide_sent[core * share + j, inner, :]

    load("table", table_hbm, table)
    load("turn", turn_hbm, turn)
    load("table_t", table_t_hbm, table_t)
    load("gate", gate_hbm.at[0], gate)
    load("taps_gate", taps_gate_hbm, taps_gate)
    load("skip", skip_hbm, skip_ref)
    load("weight", weight_hbm, weight)

    def signs(shape):
        return (1 - 2 * (lax.broadcasted_iota(jnp.int32, shape, 0) % 2)).astype(f32)

    ready("feature", "first", "second")
    used = first_hbm.shape[0]
    at = lax.broadcasted_iota(jnp.int32, first.shape, 0)
    wide = mul(feature[...], twice(jnp.where(at < used, first[...], 0.0)))
    hidden = sine(wide[:, :LANES] + wide[:, LANES:])
    wide = mul(joined(hidden, 1), twice(second_ref[...]))
    hidden = sine(wide[:, :LANES] + wide[:, LANES:])
    row_at = lax.broadcasted_iota(jnp.int32, hidden.shape, 0)
    later = jnp.where(row_at == seq_len - 1, 0.0, pltpu.roll(hidden, seq_len - 1, 0))
    ready("decay", "ahead0", "ahead1", "behind0", "behind1")
    both_rates = [decay_ref[:, lanes(me)], decay_ref[:, lanes(own_wide, share)]]
    rates = jnp.concatenate(both_rates, axis=1) * (-1.0 / (seq_len - 1))
    index = lax.broadcasted_iota(jnp.int32, (seq_len, (1 + share) * LANES), 0)
    fade = jnp.exp(rates * index.astype(f32))

    def side_of(values, w):
        high, low = split(w)
        return mul(values, jnp.concatenate([high, high], axis=0)) + mul(
            values, jnp.concatenate([low, low], axis=0)
        )

    ahead = side_of(joined(hidden, 1), ahead_w[...])
    behind = side_of(joined(later, 1), behind_w[...] * jnp.exp(rates))
    sums = (ahead + behind) * fade
    gaps = (ahead - behind) * fade
    power = jnp.sum(sums * sums + gaps * gaps, axis=0, keepdims=True) * 0.5
    scale = lax.rsqrt(power + 1e-06) * (2.0 / (2 * seq_len))
    flip = signs((seq_len, LANES)).astype(bf16)
    ready("table", "turn")
    cos_half = turn[0][:, 0:1]
    sin_half = turn[1][:, 0:1]
    def transform(j):
        cols = slice(j * LANES, (j + 1) * LANES)
        sh, sl = split(sums[:, cols])
        gh, gl = split(gaps[:, cols])

        def turned(rows_at, a, b):
            high = jnp.concatenate([a[0], b[0] * flip], axis=1)
            low = jnp.concatenate([a[1], b[1] * flip], axis=1)
            t0 = table[0, rows_at : rows_at + half, :]
            t1 = table[1, rows_at : rows_at + half, :]
            return mul(t0, high) + mul(t1, high) + mul(t0, low)

        top = turned(0, (sh, sl), (gh, gl))
        bottom = turned(half, (gh, gl), (sh, sl))
        kernel_re[j] = cos_half * top + sin_half * bottom
        kernel_im[j] = sin_half * top - cos_half * bottom

    for j in range(0):
        transform(j)
    for side in range(2):
        pl.when(inside[1 - side])(halo(side).wait_recv)
        pl.when(inside[side])(halo(side).wait_send)
    befores = halo_came[0].astype(f32)
    afters = halo_came[1].astype(f32)

    def line_of(halo, i, slab):
        return halo[slab : slab + 1, i * LANES : (i + 1) * LANES]

    rim_at = lax.broadcasted_iota(jnp.int32, (EDGE, LANES), 0)
    for slab in range(n, slabs):
        first_row = last_row = 1.0
        for i, taps in ((1, taps_mult), (2, taps_value)):
            t = taps[:, lanes(slab)]
            upper = rims[1, i, :, lanes(slab)].astype(f32)
            lower = rims[0, i, :, lanes(slab)].astype(f32)
            first_row *= (
                t[0:1] * line_of(befores, i, slab) + t[1:2] * upper[0:1] + t[2:3] * upper[1:2]
            )
            last_row *= (
                t[0:1] * lower[EDGE - 2 : EDGE - 1]
                + t[1:2] * lower[EDGE - 1 : EDGE]
                + t[2:3] * line_of(afters, i, slab)
            )
        for side, row, where in ((1, first_row, 0), (0, last_row, EDGE - 1)):
            base = 0 if side else rows - EDGE
            old = wide_sent[slab - n, base : base + EDGE, :].astype(f32)
            rim_sent[side, slab - n] = jnp.where(rim_at == where, row, old).astype(bf16)
    for peer in peers:
        for side in range(2):
            send(
                rim_sent.at[side, own_share(peer)],
                wide_came.at[:, rim_of(me, side)],
                wide_send.at[1 + side, peer],
                wide_recv.at[1 + side, me],
                peer,
            )
    for j in range(share):
        for side in range(2):
            wide_came[j, rim_of(me, side), :] = rim_sent[side, core * share + j]

    for j in range(0, 1 + share):
        transform(j)

    alternate = signs((rows, LANES))

    def convolve(j, freq):
        top, bottom = (freq[:half], freq[half:])
        kr, ki = (kernel_re[j], kernel_im[j])
        spec[j, :half] = (top * kr + bottom * ki).astype(bf16)
        spec[j, half:] = (bottom * kr - top * ki).astype(bf16)

    def invert(owner, j):
        both = mul(table_t[0, span(owner), :], spec[j])
        back = both[:, :LANES] + alternate * both[:, LANES:]
        return back * scale[:, j * LANES : (j + 1) * LANES]

    came[me] = sent[me]
    for peer in reversed(peers):
        remote(
            sent.at[peer], came.at[peer], send_sems.at[peer], recv_sems.at[peer], peer
        ).wait_recv()
    edges = [came[s, pl.ds(rows, ENDS), :].astype(f32) for s in range(n)]
    own_taps = [t[:, lanes(me)] for t in (taps_value, taps_mult)]
    pieces = []
    for s in range(n):
        top = bottom = 1.0
        for k, taps in enumerate(own_taps):
            e = edges[s][4 * k : 4 * k + 4]
            first_row = taps[1:2] * e[0:1] + taps[2:3] * e[1:2]
            last_row = taps[0:1] * e[2:3] + taps[1:2] * e[3:4]
            if s > 0:
                first_row += taps[0:1] * edges[s - 1][4 * k + 3 : 4 * k + 4]
            if s < n - 1:
                last_row += taps[2:3] * edges[s + 1][4 * k : 4 * k + 1]
            top, bottom = (top * first_row, bottom * last_row)
        block = came[s, pl.ds(0, rows), :]
        upper = jnp.where(rim_at == 0, top, block[:EDGE].astype(f32)).astype(bf16)
        lower = jnp.where(rim_at == EDGE - 1, bottom, block[rows - EDGE :].astype(f32)).astype(bf16)
        pieces += [upper, block[EDGE : rows - EDGE], lower]
    ready("table_t")
    x = jnp.concatenate(pieces, axis=0)
    convolve(0, mul(table[0], jnp.concatenate([x, x * flip], axis=1)))
    for peer in peers:
        back_sent[peer] = invert(peer, 0).astype(bf16)
        send(back_sent.at[peer], back_came.at[me], back_send.at[peer], back_recv.at[me], peer)
    own_back = invert(me, 0)

    ready("gate", "taps_gate", "skip")
    for slab in range(slabs):
        cols = lanes(slab)
        parts = []
        for i, (r, taps) in enumerate(((gate, taps_gate), (mult, taps_mult), (value, taps_value))):
            parts.append(
                short_form(
                    r[:, cols].astype(f32), taps[:, cols], line_of(befores, i, slab), line_of(afters, i, slab)
                )
            )
        gate_part[slab] = parts[0]
        direct[slab] = skip_ref[:, cols] * (parts[1] * parts[2])
    ready("weight")

    def gated(slab, convolved):
        return ((convolved + direct[slab]) * gate_part[slab]).astype(bf16)

    def project(items):
        left_side = jnp.concatenate([gated(slab, value) for slab, value in items], axis=1)
        return mul(left_side, jnp.concatenate([weight[lanes(slab), :] for slab, _ in items], axis=0))

    def returned(peer):
        remote(
            back_sent.at[peer], back_came.at[peer], back_send.at[peer], back_recv.at[peer], peer
        ).wait_recv()
        return (peer, back_came[peer].astype(f32))

    def gathered(peer):
        for i in range(3):
            where = inner_of(peer) if i == 0 else rim_of(peer, i - 1)
            what = wide_sent.at[own_share(me), inner] if i == 0 else rim_sent.at[i - 1, own_share(me)]
            remote(
                what, wide_came.at[:, where], wide_send.at[i, peer], wide_recv.at[i, peer], peer
            ).wait_recv()

    def wave(j, chip):
        where = pl.ds(pl.multiple_of(chip * rows, 2 * rows), 2 * rows)
        x = wide_came[j, where, :]
        return mul(table[0, :, where], jnp.concatenate([x, x * flip[: 2 * rows]], axis=1))

    gathered(near)
    for j in range(share):
        partial[j] = wave(j, me - core)
    for peer in reversed(far):
        gathered(peer)
    for j in range(share):
        convolve(1 + j, sum((wave(j, chip) for chip in far[::2]), partial[j]))
    for j in range(share):
        near_sent[j] = invert(near, 1 + j).astype(bf16)
    send(near_sent, near_came, near_send.at[0], near_recv.at[0], near)
    items = [(own_wide + j, invert(me, 1 + j)) for j in range(share)]
    total[...] = project(items + [(me, own_back), returned(near)])
    near_wide = n + share * (1 - core)
    items = [returned(peer) for peer in reversed(far)]
    remote(near_sent, near_came, near_send.at[0], near_recv.at[0], near).wait_recv()
    for j in range(share):
        items.append((near_wide + j, near_came[j].astype(f32)))
    out_ref[0] = (total[...] + project(items)).astype(bf16)
    for copy in copies:
        copy.wait_send()


def fused_body(n, *args):
    gate_in, mult_in, value_in, tg, tm, tv, first, second, ahead, behind, decay, skip, weight = args
    _, rows, channels = gate_in.shape
    seq_len = rows * n
    half = seq_len // 2
    width = weight.shape[1]
    slabs = channels // LANES
    share = (slabs - n) // 2
    table, table_t, turn = wave_tables(seq_len)
    table_t = table_t[:1]
    features = feature_table(seq_len, first.shape[0])
    vmem = pl.BlockSpec(memory_space=pltpu.VMEM)
    main = pl.BlockSpec(memory_space=pltpu.HBM)
    hidden_count = second.shape[0]
    dma = pltpu.SemaphoreType.DMA
    return pl.pallas_call(
        functools.partial(conv_kernel, n),
        out_shape=pltpu.VMEM((1, rows, width), bf16),
        in_specs=[main] * 17,
        out_specs=vmem,
        scratch_shapes=[
            pltpu.VMEM((2, 3, EDGE, channels), bf16),
            pltpu.VMEM((rows, channels), bf16),
            pltpu.VMEM((rows, channels), bf16),
            pltpu.VMEM((rows, channels), bf16),
            pltpu.VMEM(tg.shape, f32),
            pltpu.VMEM(tm.shape, f32),
            pltpu.VMEM(tv.shape, f32),
            pltpu.VMEM(second.shape, f32),
            pltpu.VMEM((1, channels), f32),
            pltpu.VMEM((1, channels), f32),
            pltpu.VMEM((FEATS, hidden_count), f32),
            pltpu.VMEM((hidden_count, (1 + share) * LANES), f32),
            pltpu.VMEM((hidden_count, (1 + share) * LANES), f32),
            pltpu.VMEM(weight.shape, bf16),
            pltpu.VMEM(table.shape, bf16),
            pltpu.VMEM(table_t.shape, bf16),
            pltpu.VMEM(turn.shape, f32),
            pltpu.VMEM(features.shape, bf16),
            pltpu.VMEM((2, slabs, 3 * LANES), bf16),
            pltpu.VMEM((2, slabs, 3 * LANES), bf16),
            pltpu.VMEM((n, rows + ENDS, LANES), bf16),
            pltpu.VMEM((n, rows + ENDS, LANES), bf16),
            pltpu.VMEM((2 * share, rows, LANES), bf16),
            pltpu.VMEM((2, 2 * share, EDGE, LANES), bf16),
            pltpu.VMEM((share, seq_len, LANES), bf16),
            pltpu.VMEM((n, rows, LANES), bf16),
            pltpu.VMEM((n, rows, LANES), bf16),
            pltpu.VMEM((share, rows, LANES), bf16),
            pltpu.VMEM((share, rows, LANES), bf16),
            pltpu.VMEM((1 + share, half, 2 * LANES), f32),
            pltpu.VMEM((1 + share, half, 2 * LANES), f32),
            pltpu.VMEM((1 + share, seq_len, 2 * LANES), bf16),
            pltpu.VMEM((slabs, rows, LANES), f32),
            pltpu.VMEM((slabs, rows, LANES), f32),
            pltpu.VMEM((rows, width), f32),
            pltpu.VMEM((share, seq_len, 2 * LANES), f32),
            dma((32,)),
            dma((n,)),
            dma((n,)),
            dma((3, n)),
            dma((3, n)),
            dma((n,)),
            dma((n,)),
            dma((share,)),
            dma((share,)),
            dma((2,)),
            dma((2,)),
        ],
        compiler_params=pltpu.CompilerParams(
            collective_id=0, has_side_effects=True, vmem_limit_bytes=61 * 1024 * 1024
        ),
    )(
        gate_in, mult_in, value_in, tg, tm, tv, first, second, ahead, behind,
        decay.reshape(1, channels), skip.reshape(1, channels), weight,
        jnp.asarray(table), jnp.asarray(table_t), jnp.asarray(turn), jnp.asarray(features),
    )


def body_for(n, *args):
    _, rows, channels = args[0].shape
    small = rows * n <= 1024 and rows % 128 == 0 and channels % (2 * LANES) == 0
    spare = channels // LANES > n
    network = args[6].shape[0] <= FEATS and args[6].shape[1] == 128
    if n >= 2 and n % 2 == 0 and small and spare and network and args[3].shape[0] == 3:
        return fused_body(n, *args)
    return spread_body(*args)


def solution(mesh):
    in_specs = (
        P(("grp", "row"), "col", None),
        P(("grp", "row"), "col", None),
        P(("grp", "row"), "col", None),
        P(),
        P(),
        P(),
        P(),
        P(),
        P(),
        P(),
        P(),
        P(),
        P(),
    )
    out_specs = P(("grp", "row"), "col", None)

    body = functools.partial(body_for, mesh.shape["col"])
    return jax.shard_map(body, mesh=mesh, in_specs=in_specs, out_specs=out_specs, check_vma=False)
```

```python
import functools
import math

import jax
import jax.numpy as jnp
import numpy as np
from jax import lax
from jax.experimental import pallas as pl
from jax.experimental.pallas import tpu as pltpu
from jax.sharding import PartitionSpec as P

highest = lax.Precision.HIGHEST


def padded_2(shard, sides, width):
    for axis, dim in sides:
        size, length = (lax.axis_size(axis), shard.shape[dim])
        up = [(i, (i + 1) % size) for i in range(size - 1)]
        down = [(j, i) for i, j in up]
        last = lax.slice_in_dim(shard, length - width, length, axis=dim)
        leading = lax.slice_in_dim(shard, 0, width, axis=dim)
        before = lax.ppermute(last, axis, up)
        after = lax.ppermute(leading, axis, down)
        shard = jnp.concatenate([before, shard, after], axis=dim)
    return shard


def filter_hidden(mirror, seq_len, filter_first, filter_second):
    tau_values = mirror.astype(jnp.float32) / (seq_len - 1)
    omega_pos = 2.0 * math.pi / seq_len * mirror.astype(jnp.float32)
    band_count = (filter_first.shape[0] - 1) // 2
    band_values = jnp.linspace(0.0001, band_count - 1, band_count, dtype=jnp.float32)
    angles = omega_pos[:, None] * band_values[None, :]
    features = jnp.concatenate([tau_values[:, None], jnp.cos(angles), -jnp.sin(angles)], axis=1)
    hidden = jnp.sin(jnp.dot(features, filter_first, precision=highest))
    hidden = jnp.sin(jnp.dot(hidden, filter_second, precision=highest))
    return (hidden, tau_values)


def side_values(hidden, tau_values, side_weight, decay_rates):
    values = jnp.einsum("pf,fh->hp", hidden, side_weight, precision=highest)
    return values * jnp.exp(-decay_rates[:, None] * tau_values[None, :])


def angle_table(row_count, column_count, period):
    products = (
        lax.iota(jnp.int32, row_count)[:, None]
        * lax.iota(jnp.int32, column_count)[None, :]
        % period
    )
    angle = products.astype(jnp.float32) * (2.0 * math.pi / period)
    return (jnp.cos(angle), jnp.sin(angle))


def swap_halves(stacked, width):
    return jnp.concatenate([stacked[..., width:], stacked[..., :width]], axis=-1)


def forward(values, first_table, twist_even, twist_odd, second_block):
    channels, _, width = values.shape
    first = jnp.einsum("sfa,cab->cfsb", first_table, values, precision=highest)
    first = first.reshape(channels, first_table.shape[1], 2 * width)
    turned = first * twist_even + swap_halves(first, width) * twist_odd
    return jnp.einsum("cfk,kl->cfl", turned, second_block, precision=highest)


def inverse(spectrum, last_table, twist_even, twist_odd, second_block, span_len):
    channels, freq_rows, double_width = spectrum.shape
    width = double_width // 2
    back = jnp.einsum("cfk,kl->cfl", spectrum, second_block, precision=highest)
    turned = back * twist_even + swap_halves(back, width) * twist_odd
    turned = turned.reshape(channels, freq_rows, 2, width)
    result = jnp.einsum("asf,cfsb->cab", last_table, turned, precision=highest)
    return result / span_len


def spread_body(
    gate_in,
    mult_in,
    value_in,
    taps_gate,
    taps_mult,
    taps_value,
    filter_first,
    filter_second,
    filter_ahead,
    filter_behind,
    filter_decay,
    skip_gain,
    out_weight,
):
    col_count = lax.axis_size("col")
    col_index = lax.axis_index("col")
    tok_rows = gate_in.shape[1]
    seq_len = tok_rows * col_count
    span_len = 2 * seq_len
    group_size = filter_ahead.shape[1] // col_count
    stacked = jnp.stack([gate_in[0], mult_in[0], value_in[0]])
    padded = padded_2(stacked, (("col", 1),), 1).astype(jnp.float32)
    all_taps = jnp.stack([taps_gate, taps_mult, taps_value])
    shorted = jnp.zeros(stacked.shape, jnp.float32)
    for offset in range(all_taps.shape[1]):
        shorted = shorted + all_taps[:, offset][:, None, :] * padded[:, offset : offset + tok_rows]
    gate_part = shorted[0]
    product = shorted[2] * shorted[1]
    spread = lax.all_to_all(product.T, "col", split_axis=0, concat_axis=1, tiled=True)
    first_channel = col_index * group_size
    own_rates = lax.dynamic_slice_in_dim(filter_decay, first_channel, group_size)
    mirror = lax.iota(jnp.int32, seq_len)
    hidden, tau_values = filter_hidden(mirror, seq_len, filter_first, filter_second)
    ahead_vals = side_values(
        hidden,
        tau_values,
        lax.dynamic_slice_in_dim(filter_ahead, first_channel, group_size, 1),
        own_rates,
    )
    behind_vals = side_values(
        hidden,
        tau_values,
        lax.dynamic_slice_in_dim(filter_behind, first_channel, group_size, 1),
        own_rates,
    )
    kernel = jnp.concatenate(
        [ahead_vals, jnp.zeros((group_size, 1), jnp.float32), jnp.flip(behind_vals[:, 1:], axis=1)],
        axis=1,
    )
    kernel = kernel * lax.rsqrt(jnp.sum(kernel * kernel, axis=1, keepdims=True) + 1e-06)
    factor = 128
    half_rows = factor // 2
    width_second = span_len // factor
    first_cos, first_sin = angle_table(factor, factor, factor)
    twist_cos, twist_sin = angle_table(factor, width_second, span_len)
    second_cos, second_sin = angle_table(width_second, width_second, width_second)
    first_table = jnp.stack([first_cos, -first_sin])
    last_table = jnp.stack([first_cos[:half_rows], -first_sin[:half_rows]], axis=1)
    twist_even = jnp.concatenate([twist_cos, twist_cos], axis=1)
    twist_ahead = jnp.concatenate([twist_sin, -twist_sin], axis=1)
    twist_back = jnp.concatenate([-twist_sin, twist_sin], axis=1)
    block_ahead = jnp.concatenate(
        [
            jnp.concatenate([second_cos, -second_sin], axis=1),
            jnp.concatenate([second_sin, second_cos], axis=1),
        ],
        axis=0,
    )
    block_back = jnp.concatenate(
        [
            jnp.concatenate([second_cos, second_sin], axis=1),
            jnp.concatenate([-second_sin, second_cos], axis=1),
        ],
        axis=0,
    )
    kernel_spec = forward(
        kernel.reshape(group_size, factor, width_second),
        first_table,
        twist_even,
        twist_ahead,
        block_ahead,
    )
    data_spec = forward(
        spread.reshape(group_size, half_rows, width_second),
        first_table[:, :, :half_rows],
        twist_even,
        twist_ahead,
        block_ahead,
    )
    data_re = data_spec[..., :width_second]
    data_im = data_spec[..., width_second:]
    kernel_re = kernel_spec[..., :width_second]
    kernel_im = kernel_spec[..., width_second:]
    joined = jnp.concatenate(
        [data_re * kernel_re - data_im * kernel_im, data_re * kernel_im + data_im * kernel_re],
        axis=-1,
    )
    convolved = inverse(joined, last_table, twist_even, twist_back, block_back, span_len).reshape(
        group_size, seq_len
    )
    returned = lax.all_to_all(convolved, "col", split_axis=1, concat_axis=0, tiled=True)
    mixed_rows = ((returned.T + skip_gain * product) * gate_part).astype(jnp.bfloat16)
    return jnp.dot(mixed_rows, out_weight, preferred_element_type=jnp.float32).astype(jnp.bfloat16)[
        None
    ]


f32, bf16 = (jnp.float32, jnp.bfloat16)
EDGE = 16
ENDS = 8
LANES = 128
FEATS = 64


def halves(table):
    high = table.astype(bf16)
    return [high, (table - high.astype(np.float64)).astype(bf16)]


def wave_tables(seq_len):
    odd = 2 * np.arange(seq_len, dtype=np.int64) + 1
    low = odd[: seq_len // 2]
    angle = (low[:, None] * odd[None, :] % (8 * seq_len)) * (math.pi / (4 * seq_len))
    table = np.concatenate([np.cos(angle), np.sin(angle)], axis=0)
    half = low * (math.pi / (4 * seq_len))
    turn = np.stack([np.cos(half), np.sin(half)]).astype(np.float32)
    turn = np.repeat(turn[:, :, None], LANES, axis=2)
    return (np.stack(halves(table)), np.stack(halves(table.T)), turn)


def feature_table(seq_len, feature_count):
    position = np.arange(seq_len, dtype=np.float64)
    bands = (feature_count - 1) // 2
    values = np.linspace(0.0001, bands - 1, bands)
    angles = (2.0 * math.pi / seq_len * position)[:, None] * values[None, :]
    tau = position / (seq_len - 1)
    table = np.concatenate([tau[:, None], np.cos(angles), -np.sin(angles)], axis=1)
    return np.concatenate(halves(np.pad(table, ((0, 0), (0, FEATS - feature_count)))), axis=1)


def sine(x):
    turns = jnp.floor(x * (1.0 / math.pi) + 0.5)
    r = x - turns * 3.140625
    r = r - turns * 9.67502593994140625e-4
    r = r - turns * 1.509957990978376432e-7
    sign = 1.0 - 2.0 * (turns - 2.0 * jnp.floor(turns * 0.5))
    s = r * r
    poly = 1.0 / 362880.0 - s * (1.0 / 39916800.0)
    poly = -1.0 / 5040.0 + s * poly
    poly = 1.0 / 120.0 + s * poly
    poly = -1.0 / 6.0 + s * poly
    return sign * (r + r * s * poly)


def split(value):
    high = value.astype(bf16)
    return (high, (value - high.astype(f32)).astype(bf16))


def mul(a, b):
    return jnp.dot(a, b, preferred_element_type=f32)


def joined(value, axis):
    return jnp.concatenate(split(value), axis=axis)


def twice(weight):
    both = joined(weight, 1)
    return jnp.concatenate([both, both], axis=0)


def neighbours(rows, before, after):
    count = rows.shape[0]
    index = lax.broadcasted_iota(jnp.int32, rows.shape, 0)
    up = jnp.where(index == 0, before, pltpu.roll(rows, 1, 0))
    down = jnp.where(index == count - 1, after, pltpu.roll(rows, count - 1, 0))
    return (up, down)


def short_form(rows, taps, before, after):
    up, down = neighbours(rows, before, after)
    return taps[0:1] * up + taps[1:2] * rows + taps[2:3] * down


def conv_kernel(
    n,
    gate_hbm,
    mult_hbm,
    value_hbm,
    taps_gate_hbm,
    taps_mult_hbm,
    taps_value_hbm,
    first_hbm,
    second_hbm,
    ahead_hbm,
    behind_hbm,
    decay_hbm,
    skip_hbm,
    weight_hbm,
    table_hbm,
    table_t_hbm,
    turn_hbm,
    feature_hbm,
    out_ref,
    rims,
    gate,
    mult,
    value,
    taps_gate,
    taps_mult,
    taps_value,
    second_ref,
    decay_ref,
    skip_ref,
    first,
    ahead_w,
    behind_w,
    weight,
    table,
    table_t,
    turn,
    feature,
    halo_sent,
    halo_came,
    sent,
    came,
    wide_sent,
    rim_sent,
    wide_came,
    back_sent,
    back_came,
    near_sent,
    near_came,
    kernel_re,
    kernel_im,
    spec,
    gate_part,
    direct,
    total,
    partial,
    load_sems,
    send_sems,
    recv_sems,
    wide_send,
    wide_recv,
    back_send,
    back_recv,
    near_send,
    near_recv,
    halo_send,
    halo_recv,
):
    me = lax.axis_index("col")
    rows, channels = gate.shape
    slabs = channels // LANES
    share = (slabs - n) // 2
    seq_len = rows * n
    half = seq_len // 2
    core = lax.rem(me, 2)
    near = me + 1 - 2 * core
    far = []
    for j in range(1, n // 2):
        chip = lax.rem(me - core + 2 * j, n)
        far += [chip, chip + 1]
    peers = far + [near]

    def lanes(slab, count=1):
        start = slab * LANES
        if not isinstance(slab, int):
            start = pl.multiple_of(start, LANES)
        return pl.ds(start, count * LANES)

    def span(owner):
        return pl.ds(pl.multiple_of(owner * rows, rows), rows)

    loads = {}

    def load(name, src, dst):
        copy = pltpu.make_async_copy(src, dst, load_sems.at[len(loads)])
        copy.start()
        loads[name] = copy

    def ready(*names):
        for name in names:
            loads[name].wait()

    def remote(src, dst, ssem, rsem, peer):
        return pltpu.make_async_remote_copy(
            src_ref=src,
            dst_ref=dst,
            send_sem=ssem,
            recv_sem=rsem,
            device_id={"col": peer},
            device_id_type=pl.DeviceIdType.MESH,
        )

    for side, base in enumerate((rows - EDGE, 0)):
        for i, ref in enumerate((gate_hbm, mult_hbm, value_hbm)):
            load(f"rim{side}{i}", ref.at[0, pl.ds(base, EDGE)], rims.at[side, i])
    load("taps_value", taps_value_hbm, taps_value)
    load("taps_mult", taps_mult_hbm, taps_mult)
    for i, (low, count) in enumerate(((0, n), (n, slabs - n))):
        load(f"value{i}", value_hbm.at[0, :, lanes(low, count)], value.at[:, lanes(low, count)])
        load(f"mult{i}", mult_hbm.at[0, :, lanes(low, count)], mult.at[:, lanes(low, count)])
    halo_came[...] = jnp.zeros_like(halo_came)
    barrier = pltpu.get_barrier_semaphore()
    for peer in peers:
        pl.semaphore_signal(
            barrier, inc=1, device_id={"col": peer}, device_id_type=pl.DeviceIdType.MESH
        )

    own_wide = n + share * core
    load("feature", feature_hbm, feature)
    load("first", first_hbm, first.at[pl.ds(0, first_hbm.shape[0])])
    load("second", second_hbm, second_ref)
    load("decay", decay_hbm, decay_ref)
    for name, s, d in (("ahead", ahead_hbm, ahead_w), ("behind", behind_hbm, behind_w)):
        load(name + "0", s.at[:, lanes(me)], d.at[:, lanes(0)])
        load(name + "1", s.at[:, lanes(own_wide, share)], d.at[:, lanes(1, share)])

    copies = []

    def send(*args):
        copy = remote(*args)
        copy.start()
        copies.append(copy)

    ready(*(f"rim{side}{i}" for side in range(2) for i in range(3)))
    right, left = (lax.rem(me + 1, n), lax.rem(me + n - 1, n))
    for side, at in enumerate((EDGE - 1, 0)):
        parts = []
        for i in range(3):
            line = rims[side, i].astype(f32)[at : at + 1]
            parts.append(
                jnp.concatenate([line[:, b * LANES : (b + 1) * LANES] for b in range(slabs)], axis=0)
            )
        halo_sent[side] = jnp.concatenate(parts, axis=1).astype(bf16)
    pl.semaphore_wait(barrier, n - 1)

    def halo(side):
        return remote(
            halo_sent.at[side],
            halo_came.at[side],
            halo_send.at[side],
            halo_recv.at[side],
            (right, left)[side],
        )

    inside = (me < n - 1, me > 0)
    for side in range(2):
        pl.when(inside[side])(halo(side).start)

    zero = jnp.zeros((1, LANES), f32)

    def short_product(v, m, slab):
        vs = short_form(v, taps_value[:, lanes(slab)], zero, zero)
        ms = short_form(m, taps_mult[:, lanes(slab)], zero, zero)
        product = vs * ms
        direct[slab] = product
        return product.astype(bf16)

    def pack(owner):
        v = value[:, lanes(owner)].astype(f32)
        m = mult[:, lanes(owner)].astype(f32)
        sent[owner, pl.ds(0, rows), :] = short_product(v, m, owner)
        edges = [v[0:2], v[rows - 2 : rows], m[0:2], m[rows - 2 : rows]]
        sent[owner, pl.ds(rows, ENDS), :] = jnp.concatenate(edges, axis=0).astype(bf16)

    ready("taps_value", "taps_mult", "value0", "mult0")
    for peer in peers:
        pack(peer)
        send(sent.at[peer], came.at[me], send_sems.at[peer], recv_sems.at[me], peer)
    pack(me)

    ready("value1", "mult1")
    for slab in range(n, slabs):
        cols = lanes(slab)
        wide_sent[slab - n] = short_product(value[:, cols].astype(f32), mult[:, cols].astype(f32), slab)
    inner = pl.ds(EDGE, rows - 2 * EDGE)

    def inner_of(owner):
        return pl.ds(pl.multiple_of(owner * rows + EDGE, EDGE), rows - 2 * EDGE)

    def rim_of(owner, side):
        return pl.ds(pl.multiple_of(owner * rows + (1 - side) * (rows - EDGE), EDGE), EDGE)

    def own_share(peer):
        return pl.ds(lax.rem(peer, 2) * share, share)

    for peer in peers:
        send(
            wide_sent.at[own_share(peer), inner],
            wide_came.at[:, inner_of(me)],
            wide_send.at[0, peer],
            wide_recv.at[0, me],
            peer,
        )
    for j in range(share):
        wide_came[j, inner_of(me), :] = wide_sent[core * share + j, inner, :]

    load("table", table_hbm, table)
    load("turn", turn_hbm, turn)
    load("table_t", table_t_hbm, table_t)
    load("gate", gate_hbm.at[0], gate)
    load("taps_gate", taps_gate_hbm, taps_gate)
    load("skip", skip_hbm, skip_ref)
    load("weight", weight_hbm, weight)

    def signs(shape):
        return (1 - 2 * (lax.broadcasted_iota(jnp.int32, shape, 0) % 2)).astype(f32)

    ready("feature", "first", "second")
    used = first_hbm.shape[0]
    at = lax.broadcasted_iota(jnp.int32, first.shape, 0)
    wide = mul(feature[...], twice(jnp.where(at < used, first[...], 0.0)))
    hidden = sine(wide[:, :LANES] + wide[:, LANES:])
    wide = mul(joined(hidden, 1), twice(second_ref[...]))
    hidden = sine(wide[:, :LANES] + wide[:, LANES:])
    row_at = lax.broadcasted_iota(jnp.int32, hidden.shape, 0)
    later = jnp.where(row_at == seq_len - 1, 0.0, pltpu.roll(hidden, seq_len - 1, 0))
    ready("decay", "ahead0", "ahead1", "behind0", "behind1")
    both_rates = [decay_ref[:, lanes(me)], decay_ref[:, lanes(own_wide, share)]]
    rates = jnp.concatenate(both_rates, axis=1) * (-1.0 / (seq_len - 1))
    width = (1 + share) * LANES

    def powers(count, stride):
        index = lax.broadcasted_iota(jnp.int32, (count, width), 0) * stride
        return jnp.exp(rates * index.astype(f32))

    coarse, fine = (powers(seq_len // EDGE, EDGE), powers(EDGE, 1))
    fade = jnp.concatenate([coarse[i : i + 1] * fine for i in range(seq_len // EDGE)], axis=0)

    def side_of(values, w):
        both = joined(w, 1)
        wide = mul(values, jnp.concatenate([both, both], axis=0))
        return wide[:, : w.shape[1]] + wide[:, w.shape[1] :]

    ahead = side_of(joined(hidden, 1), ahead_w[...])
    behind = side_of(joined(later, 1), behind_w[...] * jnp.exp(rates))
    sums = (ahead + behind) * fade
    gaps = (ahead - behind) * fade
    power = jnp.sum(sums * sums + gaps * gaps, axis=0, keepdims=True) * 0.5
    scale = lax.rsqrt(power + 1e-06) * (2.0 / (2 * seq_len))
    flip = signs((seq_len, LANES)).astype(bf16)
    ready("table", "turn")
    cos_half = turn[0][:, 0:1]
    sin_half = turn[1][:, 0:1]
    def transform(j):
        cols = slice(j * LANES, (j + 1) * LANES)
        sh, sl = split(sums[:, cols])
        gh, gl = split(gaps[:, cols])

        def turned(rows_at, a, b):
            high = jnp.concatenate([a[0], b[0] * flip], axis=1)
            low = jnp.concatenate([a[1], b[1] * flip], axis=1)
            t0 = table[0, rows_at : rows_at + half, :]
            t1 = table[1, rows_at : rows_at + half, :]
            return mul(t0, high) + mul(t1, high) + mul(t0, low)

        top = turned(0, (sh, sl), (gh, gl))
        bottom = turned(half, (gh, gl), (sh, sl))
        kernel_re[j] = cos_half * top + sin_half * bottom
        kernel_im[j] = sin_half * top - cos_half * bottom

    for j in range(0):
        transform(j)
    for side in range(2):
        pl.when(inside[1 - side])(halo(side).wait_recv)
        pl.when(inside[side])(halo(side).wait_send)
    befores = halo_came[0].astype(f32)
    afters = halo_came[1].astype(f32)

    def line_of(halo, i, slab):
        return halo[slab : slab + 1, i * LANES : (i + 1) * LANES]

    rim_at = lax.broadcasted_iota(jnp.int32, (EDGE, LANES), 0)
    def mend(slab):
        first_row = last_row = 1.0
        for i, taps in ((1, taps_mult), (2, taps_value)):
            t = taps[:, lanes(slab)]
            upper = rims[1, i, :, lanes(slab)].astype(f32)
            lower = rims[0, i, :, lanes(slab)].astype(f32)
            first_row *= (
                t[0:1] * line_of(befores, i, slab) + t[1:2] * upper[0:1] + t[2:3] * upper[1:2]
            )
            last_row *= (
                t[0:1] * lower[EDGE - 2 : EDGE - 1]
                + t[1:2] * lower[EDGE - 1 : EDGE]
                + t[2:3] * line_of(afters, i, slab)
            )
        for side, row, where in ((1, first_row, 0), (0, last_row, EDGE - 1)):
            base = 0 if side else rows - EDGE
            tile = jnp.where(rim_at == where, row, direct[slab, base : base + EDGE, :])
            direct[slab, base : base + EDGE, :] = tile
            if slab >= n:
                rim_sent[side, slab - n] = tile.astype(bf16)

    for slab in range(n, slabs):
        mend(slab)
    for peer in peers:
        for side in range(2):
            send(
                rim_sent.at[side, own_share(peer)],
                wide_came.at[:, rim_of(me, side)],
                wide_send.at[1 + side, peer],
                wide_recv.at[1 + side, me],
                peer,
            )
    for j in range(share):
        for side in range(2):
            wide_came[j, rim_of(me, side), :] = rim_sent[side, core * share + j]

    for j in range(0, 1 + share):
        transform(j)

    alternate = signs((rows, LANES))

    def convolve(j, freq):
        top, bottom = (freq[:half], freq[half:])
        kr, ki = (kernel_re[j], kernel_im[j])
        spec[j, :half] = (top * kr + bottom * ki).astype(bf16)
        spec[j, half:] = (bottom * kr - top * ki).astype(bf16)

    def invert(owner, j):
        both = mul(table_t[0, span(owner), :], spec[j])
        back = both[:, :LANES] + alternate * both[:, LANES:]
        return back * scale[:, j * LANES : (j + 1) * LANES]

    came[me] = sent[me]
    for peer in reversed(peers):
        remote(
            sent.at[peer], came.at[peer], send_sems.at[peer], recv_sems.at[peer], peer
        ).wait_recv()
    edges = [came[s, pl.ds(rows, ENDS), :].astype(f32) for s in range(n)]
    own_taps = [t[:, lanes(me)] for t in (taps_value, taps_mult)]
    pieces = []
    for s in range(n):
        top = bottom = 1.0
        for k, taps in enumerate(own_taps):
            e = edges[s][4 * k : 4 * k + 4]
            first_row = taps[1:2] * e[0:1] + taps[2:3] * e[1:2]
            last_row = taps[0:1] * e[2:3] + taps[1:2] * e[3:4]
            if s > 0:
                first_row += taps[0:1] * edges[s - 1][4 * k + 3 : 4 * k + 4]
            if s < n - 1:
                last_row += taps[2:3] * edges[s + 1][4 * k : 4 * k + 1]
            top, bottom = (top * first_row, bottom * last_row)
        block = came[s, pl.ds(0, rows), :]
        upper = jnp.where(rim_at == 0, top, block[:EDGE].astype(f32)).astype(bf16)
        lower = jnp.where(rim_at == EDGE - 1, bottom, block[rows - EDGE :].astype(f32)).astype(bf16)
        pieces += [upper, block[EDGE : rows - EDGE], lower]
    ready("table_t")
    x = jnp.concatenate(pieces, axis=0)
    convolve(0, mul(table[0], jnp.concatenate([x, x * flip], axis=1)))
    for peer in peers:
        back_sent[peer] = invert(peer, 0).astype(bf16)
        send(back_sent.at[peer], back_came.at[me], back_send.at[peer], back_recv.at[me], peer)
    own_back = invert(me, 0)

    ready("gate", "taps_gate", "skip")
    for slab in range(slabs):
        cols = lanes(slab)
        gate_part[slab] = short_form(
            gate[:, cols].astype(f32), taps_gate[:, cols], line_of(befores, 0, slab), line_of(afters, 0, slab)
        )
    for slab in range(n):
        mend(slab)
    ready("weight")

    def gated(slab, convolved):
        return ((convolved + skip_ref[:, lanes(slab)] * direct[slab]) * gate_part[slab]).astype(bf16)

    def project(items):
        left_side = jnp.concatenate([gated(slab, value) for slab, value in items], axis=1)
        return mul(left_side, jnp.concatenate([weight[lanes(slab), :] for slab, _ in items], axis=0))

    def returned(peer):
        remote(
            back_sent.at[peer], back_came.at[peer], back_send.at[peer], back_recv.at[peer], peer
        ).wait_recv()
        return (peer, back_came[peer].astype(f32))

    def gathered(peer):
        for i in range(3):
            where = inner_of(peer) if i == 0 else rim_of(peer, i - 1)
            what = wide_sent.at[own_share(me), inner] if i == 0 else rim_sent.at[i - 1, own_share(me)]
            remote(
                what, wide_came.at[:, where], wide_send.at[i, peer], wide_recv.at[i, peer], peer
            ).wait_recv()

    def wave(j, chip):
        where = pl.ds(pl.multiple_of(chip * rows, 2 * rows), 2 * rows)
        x = wide_came[j, where, :]
        return mul(table[0, :, where], jnp.concatenate([x, x * flip[: 2 * rows]], axis=1))

    gathered(near)
    for j in range(share):
        partial[j] = wave(j, me - core)
    for peer in reversed(far):
        gathered(peer)
    for j in range(share):
        convolve(1 + j, sum((wave(j, chip) for chip in far[::2]), partial[j]))
    for j in range(share):
        near_sent[j] = invert(near, 1 + j).astype(bf16)
    send(near_sent, near_came, near_send.at[0], near_recv.at[0], near)
    items = [(own_wide + j, invert(me, 1 + j)) for j in range(share)]
    total[...] = project(items + [(me, own_back), returned(near)])
    near_wide = n + share * (1 - core)
    items = [returned(peer) for peer in reversed(far)]
    remote(near_sent, near_came, near_send.at[0], near_recv.at[0], near).wait_recv()
    for j in range(share):
        items.append((near_wide + j, near_came[j].astype(f32)))
    out_ref[0] = (total[...] + project(items)).astype(bf16)
    for copy in copies:
        copy.wait_send()


def fused_body(n, *args):
    gate_in, mult_in, value_in, tg, tm, tv, first, second, ahead, behind, decay, skip, weight = args
    _, rows, channels = gate_in.shape
    seq_len = rows * n
    half = seq_len // 2
    width = weight.shape[1]
    slabs = channels // LANES
    share = (slabs - n) // 2
    table, table_t, turn = wave_tables(seq_len)
    table_t = table_t[:1]
    features = feature_table(seq_len, first.shape[0])
    vmem = pl.BlockSpec(memory_space=pltpu.VMEM)
    main = pl.BlockSpec(memory_space=pltpu.HBM)
    hidden_count = second.shape[0]
    dma = pltpu.SemaphoreType.DMA
    return pl.pallas_call(
        functools.partial(conv_kernel, n),
        out_shape=pltpu.VMEM((1, rows, width), bf16),
        in_specs=[main] * 17,
        out_specs=vmem,
        scratch_shapes=[
            pltpu.VMEM((2, 3, EDGE, channels), bf16),
            pltpu.VMEM((rows, channels), bf16),
            pltpu.VMEM((rows, channels), bf16),
            pltpu.VMEM((rows, channels), bf16),
            pltpu.VMEM(tg.shape, f32),
            pltpu.VMEM(tm.shape, f32),
            pltpu.VMEM(tv.shape, f32),
            pltpu.VMEM(second.shape, f32),
            pltpu.VMEM((1, channels), f32),
            pltpu.VMEM((1, channels), f32),
            pltpu.VMEM((FEATS, hidden_count), f32),
            pltpu.VMEM((hidden_count, (1 + share) * LANES), f32),
            pltpu.VMEM((hidden_count, (1 + share) * LANES), f32),
            pltpu.VMEM(weight.shape, bf16),
            pltpu.VMEM(table.shape, bf16),
            pltpu.VMEM(table_t.shape, bf16),
            pltpu.VMEM(turn.shape, f32),
            pltpu.VMEM(features.shape, bf16),
            pltpu.VMEM((2, slabs, 3 * LANES), bf16),
            pltpu.VMEM((2, slabs, 3 * LANES), bf16),
            pltpu.VMEM((n, rows + ENDS, LANES), bf16),
            pltpu.VMEM((n, rows + ENDS, LANES), bf16),
            pltpu.VMEM((2 * share, rows, LANES), bf16),
            pltpu.VMEM((2, 2 * share, EDGE, LANES), bf16),
            pltpu.VMEM((share, seq_len, LANES), bf16),
            pltpu.VMEM((n, rows, LANES), bf16),
            pltpu.VMEM((n, rows, LANES), bf16),
            pltpu.VMEM((share, rows, LANES), bf16),
            pltpu.VMEM((share, rows, LANES), bf16),
            pltpu.VMEM((1 + share, half, 2 * LANES), f32),
            pltpu.VMEM((1 + share, half, 2 * LANES), f32),
            pltpu.VMEM((1 + share, seq_len, 2 * LANES), bf16),
            pltpu.VMEM((slabs, rows, LANES), f32),
            pltpu.VMEM((slabs, rows, LANES), f32),
            pltpu.VMEM((rows, width), f32),
            pltpu.VMEM((share, seq_len, 2 * LANES), f32),
            dma((32,)),
            dma((n,)),
            dma((n,)),
            dma((3, n)),
            dma((3, n)),
            dma((n,)),
            dma((n,)),
            dma((share,)),
            dma((share,)),
            dma((2,)),
            dma((2,)),
        ],
        compiler_params=pltpu.CompilerParams(
            collective_id=0, has_side_effects=True, vmem_limit_bytes=61 * 1024 * 1024
        ),
    )(
        gate_in, mult_in, value_in, tg, tm, tv, first, second, ahead, behind,
        decay.reshape(1, channels), skip.reshape(1, channels), weight,
        jnp.asarray(table), jnp.asarray(table_t), jnp.asarray(turn), jnp.asarray(features),
    )


def body_for(n, *args):
    _, rows, channels = args[0].shape
    small = rows * n <= 1024 and rows % 128 == 0 and channels % (2 * LANES) == 0
    spare = channels // LANES > n
    network = args[6].shape[0] <= FEATS and args[6].shape[1] == 128
    if n >= 2 and n % 2 == 0 and small and spare and network and args[3].shape[0] == 3:
        return fused_body(n, *args)
    return spread_body(*args)


def solution(mesh):
    in_specs = (
        P(("grp", "row"), "col", None),
        P(("grp", "row"), "col", None),
        P(("grp", "row"), "col", None),
        P(),
        P(),
        P(),
        P(),
        P(),
        P(),
        P(),
        P(),
        P(),
        P(),
    )
    out_specs = P(("grp", "row"), "col", None)

    body = functools.partial(body_for, mesh.shape["col"])
    return jax.shard_map(body, mesh=mesh, in_specs=in_specs, out_specs=out_specs, check_vma=False)
```
